512 devices in a mesh: grp: 2 (over y), sp: 32 (over z), tp: 8 (over x, core).
Axes of the slice: x: 4, y: 2, z: 32, core: 2. Of those that a mesh axis runs over, the one named last changes fastest.
The devices are a block of a 4x8x32 slice.
Arguments:
- queries: bfloat16 [32768, 1024], P(('grp', 'sp'), 'tp'), parts along dimension 0, may hold values from -6 to 6
- memory_keys: bfloat16 [32768, 1024], P(('grp', 'sp'), 'tp'), parts along dimension 0, may hold values from -6 to 6
- memory_values: bfloat16 [32768, 1024], P(('grp', 'sp'), 'tp'), parts along dimension 0, may hold values from -6 to 6
- output_preactivation: bfloat16 [32768, 1024], P(('grp', 'sp'), 'tp'), parts along dimension 0, may hold values from -12 to 12
- input_preactivation: float32 [8, 32768], P('tp', ('grp', 'sp')), parts along dimension 1, may hold values from -6 to 140
- forget_preactivation: float32 [8, 32768], P('tp', ('grp', 'sp')), parts along dimension 1, as said below
- extra_forget_terms: float32 [8, 32768], P('tp', ('grp', 'sp')), parts along dimension 1, may hold values from -1 to 0, as said below
- head_norm_gain: float32 [128], replicated, may hold values from 0.1 to 1.9
- output_projection_matrix: bfloat16 [1024, 2048], P('tp'), may hold values from -0.1875 to 0.1875
- residual: bfloat16 [32768, 2048], P(('grp', 'sp', 'tp')), parts along dimension 0, may hold values from -6 to 6
- feedforward_norm_gain: float32 [2048], replicated, may hold values from 0.1 to 1.9
- feedforward_up_matrix: bfloat16 [2048, 8192], P('sp', 'tp'), may hold values from -0.125 to 0.125
- feedforward_down_matrix: bfloat16 [8192, 2048], P('tp', 'sp'), may hold values from -0.0625 to 0.0625
Outputs:
- layer_out: bfloat16 [32768, 2048], P(('grp', 'sp', 'tp')), parts along dimension 0
The draws below stay inside these ranges and needn't reach their ends.
There are 2 independent parts, one for each index of `grp`. The reference program is written for one: setup_inputs(seed, part) draws one part's arguments, and reference() takes and returns one part's arrays. A program takes and returns all parts, laid end to end along the dimension named above; an argument that names none is the same for every part. Nothing has to cross between parts.
Inputs may be any that keep to these rules, and one draw needn't show every extreme that they name: `forget_preactivation`: forget gate pre-activations. `extra_forget_terms`: extra log forget terms, zero at most positions.
All inputs are finite; a program needn't handle non-finite values.
Results may differ from the reference program's by a relative error of at most 0.018.
Values may be sent and summed in bfloat16 or wider, within the bound.
A program may use at most 64 MiB of HBM per device.

```python
import math
import jax
import jax.numpy as jnp
from jax import lax

D = 2048
FF = 8192
H = 8
DH = 128
BLOCK = 128
TOK_DEV = 512
M_WIDTH = 1024
SEQ = 16384
N_TP = 8


def draw_input_preactivation(key, part):
    draws = jax.random.split(jax.random.fold_in(key, 11), 1)
    values = jnp.clip(jax.random.normal(draws[0], (H, SEQ), jnp.float32), -6.0, 6.0)
    return values


def draw_forget_preactivation(key, part):
    draws = jax.random.split(jax.random.fold_in(key, 23), 3)
    order = jax.random.permutation(draws[0], H)
    slowly = order < H // 2
    center = jnp.where(slowly, math.log(2.5 * SEQ), 4.0).astype(jnp.float32)
    shifts = jax.random.uniform(draws[1], (H, SEQ // TOK_DEV, 1), jnp.float32, -0.7, 0.7)
    shifts = jnp.broadcast_to(shifts, (H, SEQ // TOK_DEV, TOK_DEV)).reshape(H, SEQ)
    jitter = jax.random.uniform(draws[2], (H, SEQ), jnp.float32, -1.0, 1.0)
    return center[:, None] + shifts + jitter


def draw_extra_forget_terms(key, part):
    draws = jax.random.split(jax.random.fold_in(key, 37), 2)
    quarter = SEQ // 4
    spots = jnp.arange(4)[None, :] * quarter + jax.random.randint(draws[0], (H, 4), 0, quarter)
    depths = jnp.log(jax.random.uniform(draws[1], (H, 4), jnp.float32, 0.5, 0.8))
    hits = jnp.arange(SEQ)[None, None, :] == spots[:, :, None]
    return jnp.sum(jnp.where(hits, depths[:, :, None], 0.0), axis=1)


def steps_of(stream_key, extent, cuts, low, top_value):
    gain, own = 1.0, jax.random.fold_in(stream_key, 6)
    for position, shards_of in cuts:
        steps = jnp.exp(jax.random.uniform(jax.random.fold_in(own, position), (shards_of,), jnp.float32, low / len(cuts), top_value / len(cuts)))
        gain = gain * jnp.repeat(steps, extent[position] // shards_of).reshape([-1 if axis == position else 1 for axis in range(len(extent))])
    return gain


def scatter_about(rng, shape, scale, reach, cuts=(), held_as=jnp.bfloat16):
    result = jax.random.normal(rng, shape, jnp.float32) * scale
    if len(cuts) > 0:
        result = steps_of(rng, shape, cuts, -0.22, 0.18) * result
    return jnp.clip(result, min=-reach, max=reach).astype(held_as)


def setup_inputs(seed: int = 0, part: int = 0) -> dict:
    key_of = jax.random.split(jax.random.key(seed), 14)
    part_splits = jax.random.split(jax.random.fold_in(key_of[13], part), 14)
    return {
        "queries": scatter_about(part_splits[0], (SEQ, M_WIDTH), 1.0, 6.0, ((0, 32), (1, 8))),
        "memory_keys": scatter_about(part_splits[1], (SEQ, M_WIDTH), 1.0, 6.0, ((0, 32), (1, 8))),
        "memory_values": scatter_about(part_splits[2], (SEQ, M_WIDTH), 1.0, 6.0, ((0, 32), (1, 8))),
        "output_preactivation": scatter_about(part_splits[3], (SEQ, M_WIDTH), 2.0, 12.0, ((0, 32), (1, 8))),
        "input_preactivation": draw_input_preactivation(jax.random.fold_in(jax.random.fold_in(key_of[13], part), 71), part),
        "forget_preactivation": draw_forget_preactivation(jax.random.fold_in(jax.random.fold_in(key_of[13], part), 71), part),
        "extra_forget_terms": draw_extra_forget_terms(jax.random.fold_in(jax.random.fold_in(key_of[13], part), 71), part),
        "head_norm_gain": jnp.clip(1.0 + 0.18 * jax.random.normal(key_of[7], (DH,), jnp.float32), 0.1, 1.9),
        "output_projection_matrix": scatter_about(key_of[8], (M_WIDTH, D), M_WIDTH ** -0.5, 0.1875, ((0, 8),)),
        "residual": scatter_about(part_splits[9], (SEQ, D), 1.0, 6.0, ((0, 256),)),
        "feedforward_norm_gain": jnp.clip(1.0 + 0.18 * jax.random.normal(key_of[10], (D,), jnp.float32), 0.1, 1.9),
        "feedforward_up_matrix": scatter_about(key_of[11], (D, FF), D ** -0.5, 0.125, ((0, 32), (1, 8))),
        "feedforward_down_matrix": scatter_about(key_of[12], (FF, D), FF ** -0.5, 0.0625, ((0, 8), (1, 32))),
    }


neg_big = -1e+30
norm_eps = 1e-06
highest = lax.Precision.HIGHEST

def rms_norm(tensor, gain_vec):
    mean_sq = lax.optimization_barrier(jnp.mean(tensor * tensor, axis=-1, keepdims=True))
    return tensor * lax.rsqrt(mean_sq + norm_eps) * gain_vec

def memory_cell(queries, memory_keys, memory_values, input_preactivation, forget_logarithm):
    blocks = SEQ // BLOCK

    def to_blocks(tensor):
        return jnp.moveaxis(tensor.reshape((H, blocks, BLOCK) + tensor.shape[2:]), 1, 0)
    causal = jnp.arange(BLOCK)[:, None] >= jnp.arange(BLOCK)[None, :]

    def advance(state_now, pieces):
        memory, stab_max = state_now
        query_blk, key_blk, val_blk, gate_blk, fgt_blk = pieces
        decay_logarithm = jnp.cumsum(fgt_blk, axis=-1)
        log_weight = decay_logarithm[:, :, None] - decay_logarithm[:, None, :] + gate_blk[:, None, :]
        log_weight = jnp.where(causal, log_weight, neg_big)
        carry_log = decay_logarithm + stab_max[:, None]
        row_max = jnp.maximum(lax.optimization_barrier(jnp.max(log_weight, axis=-1)), carry_log)
        scores = jnp.einsum('htd,hsd->hts', query_blk, key_blk, precision=highest) * jnp.exp(log_weight - row_max[..., None])
        carry_scale = jnp.exp(carry_log - row_max)
        hidden = jnp.einsum('hts,hsv->htv', scores, val_blk, precision=highest)
        hidden = hidden + carry_scale[..., None] * jnp.einsum('hvk,htk->htv', memory, query_blk, precision=highest)
        block_total = decay_logarithm[:, -1]
        tail_log = block_total[:, None] - decay_logarithm + gate_blk
        new_max = jnp.maximum(block_total + stab_max, lax.optimization_barrier(jnp.max(tail_log, axis=-1)))
        weights = jnp.exp(tail_log - new_max[:, None])
        carry_decay = jnp.exp(block_total + stab_max - new_max)
        memory = carry_decay[:, None, None] * memory + jnp.einsum('hs,hsv,hsk->hvk', weights, val_blk, key_blk, precision=highest)
        return ((memory, new_max), hidden)
    start_state = (jnp.zeros((H, DH, DH), jnp.float32), jnp.zeros((H,), jnp.float32))
    pieces = (to_blocks(queries), to_blocks(memory_keys), to_blocks(memory_values), to_blocks(input_preactivation), to_blocks(forget_logarithm))
    _, results = lax.scan(advance, start_state, pieces)
    return jnp.moveaxis(results, 0, 1).reshape(H, SEQ, DH)

def to_heads(tensor):
    return tensor.astype(jnp.float32).reshape(SEQ, H, DH).transpose(1, 0, 2)

def reference(queries, memory_keys, memory_values, output_preactivation, input_preactivation, forget_preactivation, extra_forget_terms, head_norm_gain, output_projection_matrix, residual, feedforward_norm_gain, feedforward_up_matrix, feedforward_down_matrix):
    forget_logarithm = jax.nn.log_sigmoid(forget_preactivation) + extra_forget_terms
    hidden = memory_cell(to_heads(queries), to_heads(memory_keys) * DH ** (-0.5), to_heads(memory_values), input_preactivation, forget_logarithm)
    hidden = hidden.transpose(1, 0, 2)
    gated = rms_norm(hidden, head_norm_gain) * jax.nn.sigmoid(output_preactivation.astype(jnp.float32).reshape(SEQ, H, DH))
    mixed = gated.reshape(SEQ, H * DH).astype(jnp.bfloat16)
    width_tp = H * DH // N_TP
    branch = jnp.zeros((SEQ, D), jnp.float32)
    for group_idx in range(N_TP):
        lower_col = group_idx * width_tp
        partial_value = jnp.dot(mixed[:, lower_col:lower_col + width_tp], output_projection_matrix[lower_col:lower_col + width_tp], preferred_element_type=jnp.float32)
        branch = branch + lax.optimization_barrier(partial_value.astype(jnp.bfloat16)).astype(jnp.float32)
    mid_state = (residual.astype(jnp.float32) + branch).astype(jnp.bfloat16)
    normed = rms_norm(mid_state.astype(jnp.float32), feedforward_norm_gain).astype(jnp.bfloat16)
    ff_tp = FF // N_TP
    mlp_sum = jnp.zeros((SEQ, D), jnp.float32)
    for group_idx in range(N_TP):
        lower_col = group_idx * ff_tp
        upward = jnp.dot(normed, feedforward_up_matrix[:, lower_col:lower_col + ff_tp], preferred_element_type=jnp.float32)
        active = jnp.square(jax.nn.relu(upward)).astype(jnp.bfloat16)
        partial_value = jnp.dot(active, feedforward_down_matrix[lower_col:lower_col + ff_tp], preferred_element_type=jnp.float32)
        mlp_sum = mlp_sum + lax.optimization_barrier(partial_value.astype(jnp.bfloat16)).astype(jnp.float32)
    return (mid_state.astype(jnp.float32) + mlp_sum).astype(jnp.bfloat16)
```

```python
import functools

import jax
import jax.numpy as jnp
from jax import lax
from jax.experimental import pallas as pl
from jax.experimental.pallas import tpu as pltpu
from jax.sharding import PartitionSpec as P

BLOCK = 128
CORES = 2
SUB = 4
UNIT = 16
NORM_EPS = 1e-06
NEG_BIG = -1e30
MESH = pl.DeviceIdType.MESH
F32 = jnp.float32
BF16 = jnp.bfloat16


def two_part_dot(a, b, dims=(((1,), (0,)), ((), ()))):
    high = a.astype(BF16)
    low = (a - high.astype(F32)).astype(BF16)
    dot = functools.partial(lax.dot_general, dimension_numbers=dims, preferred_element_type=F32)
    return dot(high, b) + dot(low, b)


def dot_two_part(a, b):
    high = b.astype(BF16)
    low = (b - high.astype(F32)).astype(BF16)
    return jnp.dot(a, high, preferred_element_type=F32) + jnp.dot(a, low, preferred_element_type=F32)


def rem(a, b):
    return lax.rem(a, jnp.int32(b))


def kernel(
    sizes,
    q_ref, k_ref, v_ref, og_ref, ig_ref, fg_ref, ex_ref, hng_ref, wo_in, res_in, fng_ref, up_in, dn_in,
    out_ref,
    UP, DN, WO, RES, MIX, MID, NRM, SSQ, ACT, PART, SIB, SUM, RSR, LM, ST, AS, AR, GX, BS, BR, CS, CR,
    SR, RR, SL, RL, SY, RYU, RYD, SX, RX, SD, RD, SA, RA, SB, RB, SC, RC, SP, RP, SQ, RQ,
):
    nz, nt, share = sizes
    nx = nt // CORES
    ng = nz // SUB
    n_right, n_left = nz // 2, nz - 1 - nz // 2
    tok, dh = q_ref.shape
    nb = tok // BLOCK
    width = res_in.shape[1]
    own_rows = res_in.shape[0]
    wrows, hid = up_in.shape
    gcols = SUB * wrows

    me, t, grp = lax.axis_index("sp"), lax.axis_index("tp"), lax.axis_index("grp")
    x, c = lax.div(t, jnp.int32(CORES)), rem(t, CORES)
    sib = x * CORES + 1 - c
    parity = rem(grp, 2)
    pair = grp + 1 - 2 * parity
    right, left = rem(me + 1, nz), rem(me + nz - 1, nz)
    gz, j = lax.div(me, jnp.int32(SUB)), rem(me, SUB)

    def remote(src, dst, send, recv, **device):
        return pltpu.make_async_remote_copy(
            src_ref=src, dst_ref=dst, send_sem=send, recv_sem=recv, device_id=device, device_id_type=MESH
        )

    def drain(ref, sem):
        pltpu.make_async_copy(ref, ref, sem).wait()

    barrier = pltpu.get_barrier_semaphore()
    others = [dict(sp=right), dict(sp=left), dict(sp=rem(me + SUB, nz)), dict(sp=rem(me + nz - SUB, nz))]
    others += [dict(sp=gz * SUB + rem(j + d, SUB)) for d in range(1, SUB)]
    others += [dict(tp=rem(x + d, nx) * CORES + c) for d in range(1, nx)]
    others += [dict(tp=sib)]
    if share:
        others += [dict(grp=pair)]
    for device in others:
        pl.semaphore_signal(barrier, inc=1, device_id=device, device_id_type=MESH)
    pl.semaphore_wait(barrier, len(others))

    if share:
        offsets = [2 * UNIT, 3 * UNIT, parity * UNIT]
    else:
        offsets = [0, UNIT, 2 * UNIT, 3 * UNIT]
    n_pieces = len(offsets)
    weights, own_w = (UP, DN), (up_in, dn_in)

    def piece(ph, origin, i):
        return weights[ph].at[pl.ds(pl.multiple_of(origin * wrows + offsets[i], UNIT), UNIT), :]

    def hop0(ph):
        for i in range(n_pieces):
            src = own_w[ph].at[pl.ds(pl.multiple_of(offsets[i] + 0 * me, UNIT), UNIT), :]
            remote(src, piece(ph, me, i), SR.at[ph, i], RR.at[ph, i, 1], sp=right).start()
            remote(src, piece(ph, me, i), SL.at[ph, i], RL.at[ph, i, 1], sp=left).start()

    def to_pair(ph, origin):
        if ph == 0:
            sem = RYU.at[0]
        else:
            sem = RYD.at[rem(lax.div(origin, jnp.int32(SUB)) - gz + ng, ng)]
        part = piece(ph, origin, n_pieces - 1)
        remote(part, part, SY.at[ph], sem, grp=pair).start()

    def tick(ph, h):
        from_left, from_right = rem(me - h + nz, nz), rem(me + h, nz)
        for i in reversed(range(n_pieces)):
            a, b = piece(ph, from_left, i), piece(ph, from_right, i)
            remote(a, a, SR.at[ph, i], RR.at[ph, i, h], sp=right).wait_recv()

            @pl.when(h < n_right)
            def _():
                remote(a, a, SR.at[ph, i], RR.at[ph, i, h + 1], sp=right).start()

            if share and i == n_pieces - 1:
                to_pair(ph, from_left)

            @pl.when(h <= n_left)
            def _():
                remote(b, b, SL.at[ph, i], RL.at[ph, i, h], sp=left).wait_recv()

                @pl.when(h < n_left)
                def _():
                    remote(b, b, SL.at[ph, i], RL.at[ph, i, h + 1], sp=left).start()

                if share and i == n_pieces - 1:
                    to_pair(ph, from_right)

    def ticks(ph, first, last):
        def body(h, _):
            tick(ph, h)
            return 0

        lax.fori_loop(first, last + 1, body, 0)

    hop0(0)

    waits = []

    def wo_rows(s):
        return WO.at[pl.ds(pl.multiple_of(s * dh, dh), dh), :]

    def res_rows(s):
        return RES.at[pl.ds(pl.multiple_of(s * own_rows, own_rows), own_rows), :]

    def mix_cols(s):
        return MIX.at[:, pl.ds(pl.multiple_of(s * dh, dh), dh)]

    def spread(which, own, region):
        for d in [2, 1, 3, *range(4, nx)]:
            if d < nx:
                copy = remote(own, region(t), SX.at[which, d], RX.at[which, d], tp=rem(x + d, nx) * CORES + c)
                copy.start()
                waits.append(copy)
        copy = remote(own, region(t), SD.at[which, 0], RD.at[which, 0], tp=sib)
        copy.start()
        waits.append(copy)

    def pass_on(which, region):
        for d in range(1, nx):
            part = region(rem(x - d + nx, nx) * CORES + c)
            remote(part, part, SX.at[which, d], RX.at[which, d], tp=sib).wait_recv()
            copy = remote(part, part, SD.at[which, d], RD.at[which, d], tp=sib)
            copy.start()
            waits.append(copy)

    def passed(which, region):
        for d in range(nx):
            part = region(rem(x - d + nx, nx) * CORES + 1 - c)
            remote(part, part, SD.at[which, d], RD.at[which, d], tp=sib).wait_recv()

    spread(0, res_in, res_rows)
    spread(1, wo_in, wo_rows)

    lane = lax.broadcasted_iota(jnp.int32, (1, BLOCK), 1)
    scale = dh ** (-0.5)
    total = top = memory = None
    for b in range(nb):
        cols = slice(b * BLOCK, (b + 1) * BLOCK)
        f = fg_ref[:, cols]
        cum = jnp.minimum(f, 0.0) - jnp.log1p(jnp.exp(-jnp.abs(f))) + ex_ref[:, cols]
        step = 1
        while step < BLOCK:
            cum = cum + jnp.where(lane >= step, pltpu.roll(cum, step, 1), 0.0)
            step *= 2
        ST[b : b + 1, :] = cum
        whole = jnp.sum(jnp.where(lane == BLOCK - 1, cum, 0.0), axis=1, keepdims=True)
        tail = whole - cum + ig_ref[:, cols]
        tail_top = jnp.max(tail, axis=1, keepdims=True)
        weight = jnp.exp(tail - tail_top)
        keys_t = k_ref[cols, :].astype(F32).T
        part = two_part_dot(keys_t * weight, v_ref[cols, :]) * scale
        if b == 0:
            total, top, memory = whole, tail_top, part
        else:
            LM[b - 1] = memory
            ST[8 + b : 9 + b, :] = jnp.broadcast_to(total, (1, BLOCK))
            ST[16 + b : 17 + b, :] = jnp.broadcast_to(top, (1, BLOCK))
            new_top = jnp.maximum(whole + top, tail_top)
            memory = jnp.exp(whole + top - new_top) * memory + jnp.exp(tail_top - new_top) * part
            total, top = total + whole, new_top
    srows = dh // SUB
    for i in range(SUB):
        AS[i, 0:srows, :] = memory[i * srows : (i + 1) * srows, :]
        AS[i, srows : srows + 1, :] = jnp.broadcast_to(total, (1, dh))
        AS[i, srows + 1 : srows + 2, :] = jnp.broadcast_to(top, (1, dh))
    for d in range(1, SUB):
        i = rem(j + d, SUB)
        copy = remote(AS.at[i], AR.at[j], SA.at[d], RA.at[d], sp=gz * SUB + i)
        copy.start()
        waits.append(copy)
    AR[j] = AS[j]
    UP[pl.ds(pl.multiple_of(me * wrows, wrows), wrows), :] = up_in[...]
    DN[pl.ds(pl.multiple_of(me * wrows, wrows), wrows), :] = dn_in[...]
    WO[pl.ds(pl.multiple_of(t * dh, dh), dh), :] = wo_in[...]
    RES[pl.ds(pl.multiple_of(t * own_rows, own_rows), own_rows), :] = res_in[...]

    first = n_right - 2 * (ng - 1)
    ticks(0, 1, first)
    for d in range(1, SUB):
        slot = AR.at[rem(j - d + SUB, SUB)]
        remote(slot, slot, SA.at[d], RA.at[d], sp=right).wait_recv()

    def member(i):
        return AR[i, 0:srows, :], AR[i, srows : srows + 1, :], AR[i, srows + 1 : srows + 2, :]

    def fold(state, top, member_state):
        part, part_total, part_top = member_state
        new_top = jnp.maximum(part_total + top, part_top)
        return jnp.exp(part_total + top - new_top) * state + jnp.exp(part_top - new_top) * part, new_top

    g_state, g_total, g_top = member(0)
    for i in range(1, SUB):
        m_state = member(i)
        g_state, g_top = fold(g_state, g_top, m_state)
        g_total = g_total + m_state[1]
    GX[0:srows, :] = g_state
    GX[srows : srows + 1, :] = g_total
    GX[srows + 1 : srows + 2, :] = g_top

    def chain(r):
        @pl.when(gz == r)
        def _():
            @pl.when(gz > 0)
            def _():
                remote(BR, BR, SB.at[0], RB.at[0], sp=right).wait_recv()

            @pl.when(gz == 0)
            def _():
                BR[...] = jnp.zeros_like(BR)

            state, top = BR[0:srows, :], BR[srows + 1 : srows + 2, :]
            after, after_top = fold(
                state, top, (GX[0:srows, :], GX[srows : srows + 1, :], GX[srows + 1 : srows + 2, :])
            )
            BS[0:srows, :] = after
            BS[srows + 1 : srows + 2, :] = after_top

            @pl.when(gz < ng - 1)
            def _():
                remote(BS, BR, SB.at[0], RB.at[0], sp=rem(me + SUB, nz)).start()

            for i in range(SUB):
                CS[i, 0:srows, :] = state
                CS[i, srows + 1 : srows + 2, :] = top
                if i < SUB - 1:
                    state, top = fold(state, top, member(i))
            for d in range(1, SUB):
                i = rem(j + d, SUB)
                remote(CS.at[i], CR.at[j], SC.at[d], RC.at[d], sp=gz * SUB + i).start()
            CR[j] = CS[j]

    def chain_step(r, _):
        chain(r)
        tick(0, first + 1 + 2 * r)
        tick(0, first + 2 + 2 * r)
        return 0

    lax.fori_loop(0, ng - 2, chain_step, 0)
    hop0(1)
    chain_step(ng - 2, 0)
    chain(ng - 1)
    pass_on(0, res_rows)
    pass_on(1, wo_rows)
    tick(1, 1)

    for d in range(1, SUB):
        slot = CR.at[rem(j - d + SUB, SUB)]
        remote(slot, slot, SC.at[d], RC.at[d], sp=right).wait_recv()
    before = jnp.concatenate([CR[i, 0:srows, :] for i in range(SUB)], axis=0)
    before_top = CR[0, srows + 1 : srows + 2, :]
    causal = lax.broadcasted_iota(jnp.int32, (BLOCK, BLOCK), 0) >= lax.broadcasted_iota(
        jnp.int32, (BLOCK, BLOCK), 1
    )
    mine = pl.ds(pl.multiple_of(t * dh, dh), dh)
    for b in range(nb):
        cols = slice(b * BLOCK, (b + 1) * BLOCK)
        cum = ST[b : b + 1, :]
        if b == 0:
            start, start_top = before, before_top
        else:
            total, top = ST[8 + b : 9 + b, :], ST[16 + b : 17 + b, :]
            start_top = jnp.maximum(total + before_top, top)
            start = jnp.exp(total + before_top - start_top) * before + jnp.exp(top - start_top) * LM[b - 1]
        cum_t = jnp.broadcast_to(cum, (BLOCK, BLOCK)).T
        log_weight = jnp.where(causal, cum_t - cum + ig_ref[:, cols], NEG_BIG)
        carry_log = cum_t + start_top
        row_max = jnp.maximum(jnp.max(log_weight, axis=1, keepdims=True), carry_log)
        q, k, v = q_ref[cols, :], k_ref[cols, :], v_ref[cols, :]
        qk = lax.dot_general(q, k, (((1,), (1,)), ((), ())), preferred_element_type=F32) * scale
        hidden = two_part_dot(qk * jnp.exp(log_weight - row_max), v)
        hidden = hidden + jnp.exp(carry_log - row_max) * dot_two_part(q, start)
        mean_sq = jnp.mean(hidden * hidden, axis=1, keepdims=True)
        gate = jax.nn.sigmoid(og_ref[cols, :].astype(F32))
        mixed = hidden * lax.rsqrt(mean_sq + NORM_EPS) * hng_ref[...] * gate
        MIX[cols, mine] = mixed.astype(BF16)
    spread(2, mix_cols(t), mix_cols)
    ticks(1, 2, 4)
    pass_on(2, mix_cols)
    for which, region in ((0, res_rows), (1, wo_rows)):
        passed(which, region)
    tick(1, 5)
    passed(2, mix_cols)

    SSQ[...] = jnp.zeros_like(SSQ)

    def project(n, _):
        at = pl.ds(pl.multiple_of(n * 256, 256), 256)
        branch = jnp.dot(MIX[...], WO[:, at], preferred_element_type=F32)
        mid = (RES[:, at].astype(F32) + branch).astype(BF16)
        MID[:, at] = mid
        wide = mid.astype(F32)
        SSQ[...] += wide[:, :128] * wide[:, :128] + wide[:, 128:] * wide[:, 128:]
        return 0

    n_cols = width // 256
    for n in range(0, n_cols, 4):
        lax.fori_loop(n, n + 4, project, 0)
        tick(1, 6 + n // 4)

    def normalize(n, _):
        at = pl.ds(pl.multiple_of(n * 64, 64), 64)
        mean_sq = jnp.sum(SSQ[at, :], axis=1, keepdims=True) / width
        NRM[at, :] = (MID[at, :].astype(F32) * lax.rsqrt(mean_sq + NORM_EPS) * fng_ref[...]).astype(BF16)
        return 0

    lax.fori_loop(0, tok // 64, normalize, 0)
    tick(1, 8)

    if share:
        drain(UP.at[pl.ds(0, (nz - 1) * UNIT), :], RYU.at[0])

    def upward(n, _):
        at = pl.ds(pl.multiple_of(n * 256, 256), 256)
        value = jnp.maximum(jnp.dot(NRM[...], UP[:, at], preferred_element_type=F32), 0.0)
        ACT[:, at] = (value * value).astype(BF16)
        return 0

    for n in range(0, hid // 256, 2):
        lax.fori_loop(n, n + 2, upward, 0)
        tick(1, 9 + n // 2)

    def group_of(k):
        return rem(gz + k, ng)

    def down(k):
        if share:
            drain(DN.at[pl.ds(0, (SUB if k else SUB - 1) * UNIT), :], RYD.at[k])
        rows = pl.ds(pl.multiple_of(group_of(k) * gcols, gcols), gcols)
        value = lax.dot_general(
            ACT[...], DN[rows, :], (((1,), (1,)), ((), ())), preferred_element_type=F32
        )
        PART[k] = value.astype(BF16).reshape(nx, CORES, own_rows, gcols)
        copy = remote(PART.at[k, :, 1 - c], SIB.at[k], SP.at[k], RP.at[k], tp=sib)
        copy.start()
        waits.append(copy)

    def add_up(k):
        remote(SIB.at[k], SIB.at[k], SP.at[k], RP.at[k], tp=sib).wait_recv()
        for i in range(nx):
            SUM[k, i] = (PART[k, i, c].astype(F32) + SIB[k, i].astype(F32)).astype(BF16)
        for d in [2, 1, 3, *range(4, nx)]:
            if d < nx:
                i = rem(x + d, nx)
                copy = remote(SUM.at[k, i], RSR.at[k, x], SQ.at[k, d], RQ.at[k, d], tp=i * CORES + c)
                copy.start()
                waits.append(copy)

    def finish(k):
        at = pl.ds(pl.multiple_of(group_of(k) * gcols, gcols), gcols)
        value = MID[pl.ds(pl.multiple_of(t * own_rows, own_rows), own_rows), at].astype(F32)
        value = value + SUM[k, x].astype(F32)
        for d in range(1, nx):
            slot = RSR.at[k, rem(x - d + nx, nx)]
            remote(slot, slot, SQ.at[k, d], RQ.at[k, d], tp=sib).wait_recv()
            value = value + RSR[k, rem(x - d + nx, nx)].astype(F32)
        out_ref[:, at] = value.astype(BF16)

    done, order = 8 + hid // 512, []
    plan = [(0, 3)]
    for s in range(1, ng // 2):
        plan += [(ng - s, SUB * s + 3), (s, SUB * s + 3)]
    plan += [(ng // 2, n_right)]
    late = 0
    for n, (k, need) in enumerate(plan):
        while done < need:
            done += 1
            tick(1, done)
        down(k)
        if done < n_right and n < len(plan) - 1 and done < 14:
            done += 1
            tick(1, done)
        order.append(k)
        if n > 0:
            add_up(order[n - 1])
        if n > 3:
            finish(order[late])
            late += 1
    add_up(order[-1])
    for k in order[late:]:
        finish(k)

    for ph in range(2):
        for i in range(n_pieces):
            drain(weights[ph].at[pl.ds(0, n_right * UNIT), :], SR.at[ph, i])
            drain(weights[ph].at[pl.ds(0, n_left * UNIT), :], SL.at[ph, i])
        if share:
            drain(weights[ph].at[pl.ds(0, (nz - 1) * UNIT), :], SY.at[ph])
    for copy in waits:
        copy.wait_send()
    for d in range(1, SUB):
        drain(CS.at[0], SC.at[d])

    @pl.when(gz < ng - 1)
    def _():
        drain(BS, SB.at[0])


def shards(
    sizes,
    queries,
    memory_keys,
    memory_values,
    output_preactivation,
    input_preactivation,
    forget_preactivation,
    extra_forget_terms,
    head_norm_gain,
    output_projection_matrix,
    residual,
    feedforward_norm_gain,
    feedforward_up_matrix,
    feedforward_down_matrix,
):
    nz, nt, share = sizes
    nx, ng = nt // CORES, nz // SUB
    tok, dh = queries.shape
    own_rows, width = residual.shape
    wrows, hid = feedforward_up_matrix.shape
    n_right = nz // 2
    n_pieces = 3 if share else 4
    gcols = SUB * wrows
    msg = (dh // SUB + 8, dh)
    dma = pltpu.SemaphoreType.DMA
    vmem = pltpu.VMEM
    scratch = [
        vmem((nz * wrows, hid), BF16),
        vmem((nz * wrows, hid), BF16),
        vmem((nt * dh, width), BF16),
        vmem((tok, width), BF16),
        vmem((tok, nt * dh), BF16),
        vmem((tok, width), BF16),
        vmem((tok, width), BF16),
        vmem((tok, 128), F32),
        vmem((tok, hid), BF16),
        vmem((ng, nx, CORES, own_rows, gcols), BF16),
        vmem((ng, nx, own_rows, gcols), BF16),
        vmem((ng, nx, own_rows, gcols), BF16),
        vmem((ng, nx, own_rows, gcols), BF16),
        vmem((tok // BLOCK - 1, dh, dh), F32),
        vmem((24, BLOCK), F32),
        vmem((SUB, *msg), F32),
        vmem((SUB, *msg), F32),
        vmem(msg, F32),
        vmem(msg, F32),
        vmem(msg, F32),
        vmem((SUB, *msg), F32),
        vmem((SUB, *msg), F32),
        dma((2, n_pieces)),
        dma((2, n_pieces, n_right + 1)),
        dma((2, n_pieces)),
        dma((2, n_pieces, n_right + 1)),
        dma((2,)),
        dma((1,)),
        dma((ng,)),
        dma((3, nx)),
        dma((3, nx)),
        dma((3, nx)),
        dma((3, nx)),
        dma((SUB,)),
        dma((SUB,)),
        dma((1,)),
        dma((1,)),
        dma((SUB,)),
        dma((SUB,)),
        dma((ng,)),
        dma((ng,)),
        dma((ng, nx)),
        dma((ng, nx)),
    ]
    return pl.pallas_call(
        functools.partial(kernel, sizes),
        out_shape=jax.ShapeDtypeStruct((own_rows, width), BF16),
        in_specs=[pl.BlockSpec(memory_space=pltpu.VMEM)] * 13,
        out_specs=pl.BlockSpec(memory_space=pltpu.VMEM),
        scratch_shapes=scratch,
        compiler_params=pltpu.CompilerParams(
            collective_id=0, has_side_effects=True, vmem_limit_bytes=56 * 1024 * 1024
        ),
        name="layer",
    )(
        queries,
        memory_keys,
        memory_values,
        output_preactivation,
        input_preactivation,
        forget_preactivation,
        extra_forget_terms,
        head_norm_gain.reshape(1, -1),
        output_projection_matrix,
        residual,
        feedforward_norm_gain.reshape(1, -1),
        feedforward_up_matrix,
        feedforward_down_matrix.T,
    )


def solution(mesh):
    in_specs = (
        P(("grp", "sp"), "tp"),
        P(("grp", "sp"), "tp"),
        P(("grp", "sp"), "tp"),
        P(("grp", "sp"), "tp"),
        P("tp", ("grp", "sp")),
        P("tp", ("grp", "sp")),
        P("tp", ("grp", "sp")),
        P(),
        P("tp", None),
        P(("grp", "sp", "tp"), None),
        P(),
        P("sp", "tp"),
        P("tp", "sp"),
    )
    out_specs = P(("grp", "sp", "tp"), None)
    sizes = (mesh.shape["sp"], mesh.shape["tp"], mesh.shape["grp"] % 2 == 0)
    return jax.shard_map(
        functools.partial(shards, sizes), mesh=mesh, in_specs=in_specs, out_specs=out_specs, check_vma=False
    )
```

```python
import functools

import jax
import jax.numpy as jnp
from jax import lax
from jax.experimental import pallas as pl
from jax.experimental.pallas import tpu as pltpu
from jax.sharding import PartitionSpec as P

BLOCK = 128
CHAIN_LATE = 7
CORES = 2
SUB = 4
UNIT = 16
NORM_EPS = 1e-06
NEG_BIG = -1e30
MESH = pl.DeviceIdType.MESH
F32 = jnp.float32
BF16 = jnp.bfloat16


def two_part_dot(a, b, dims=(((1,), (0,)), ((), ()))):
    high = a.astype(BF16)
    low = (a - high.astype(F32)).astype(BF16)
    dot = functools.partial(lax.dot_general, dimension_numbers=dims, preferred_element_type=F32)
    return dot(high, b) + dot(low, b)


def dot_two_part(a, b):
    high = b.astype(BF16)
    low = (b - high.astype(F32)).astype(BF16)
    return jnp.dot(a, high, preferred_element_type=F32) + jnp.dot(a, low, preferred_element_type=F32)


def rem(a, b):
    return lax.rem(a, jnp.int32(b))


def kernel(
    sizes,
    q_ref, k_ref, v_ref, og_ref, ig_ref, fg_ref, ex_ref, hng_ref, wo_in, res_in, fng_ref, up_in, dn_in,
    out_ref,
    UP, DN, WO, RES, MIX, MID, NRM, SSQ, UACC, ACT, PART, SIB, SUM, RSR, LM, ST, AS, AR, GX, BS, BR, CS, CR,
    SR, RR, SL, RL, SY, RY, SX, RX, SD, RD, SA, RA, SB, RB, SC, RC, SP, RP, SQ, RQ,
):
    nz, nt, share = sizes
    nx = nt // CORES
    ng = nz // SUB
    n_right, n_left = nz // 2, nz - 1 - nz // 2
    tok, dh = q_ref.shape
    nb = tok // BLOCK
    width = res_in.shape[1]
    own_rows = res_in.shape[0]
    wrows, hid = up_in.shape
    gcols = SUB * wrows

    me, t, grp = lax.axis_index("sp"), lax.axis_index("tp"), lax.axis_index("grp")
    x, c = lax.div(t, jnp.int32(CORES)), rem(t, CORES)
    sib = x * CORES + 1 - c
    parity = rem(grp, 2)
    pair = grp + 1 - 2 * parity
    right, left = rem(me + 1, nz), rem(me + nz - 1, nz)
    gz, j = lax.div(me, jnp.int32(SUB)), rem(me, SUB)

    def remote(src, dst, send, recv, **device):
        return pltpu.make_async_remote_copy(
            src_ref=src, dst_ref=dst, send_sem=send, recv_sem=recv, device_id=device, device_id_type=MESH
        )

    def drain(ref, sem):
        pltpu.make_async_copy(ref, ref, sem).wait()

    barrier = pltpu.get_barrier_semaphore()
    others = [dict(sp=right), dict(sp=left), dict(sp=rem(me + SUB, nz)), dict(sp=rem(me + nz - SUB, nz))]
    others += [dict(sp=gz * SUB + rem(j + d, SUB)) for d in range(1, SUB)]
    others += [dict(tp=rem(x + d, nx) * CORES + c) for d in range(1, nx)]
    others += [dict(tp=sib)]
    if share:
        others += [dict(grp=pair)]
    for device in others:
        pl.semaphore_signal(barrier, inc=1, device_id=device, device_id_type=MESH)
    pl.semaphore_wait(barrier, len(others))

    hid_half = hid // 2
    if share:
        mine_row, mine_col = parity * UNIT, parity * hid_half
        cuts = (
            [(3 * UNIT, 0, hid, False), (2 * UNIT, mine_col, hid_half, True), (mine_row, 0, hid, True)],
            [(2 * UNIT, 0, hid, False), (3 * UNIT, 0, hid, False), (mine_row, 0, hid, True)],
        )
        order = [(0, 2), (1, 2), (0, 1), (1, 1), (0, 0), (1, 0)]
    else:
        cuts = ([(i * UNIT, 0, hid, False) for i in range(4)],) * 2
        order = [(ph, i) for i in range(4) for ph in range(2)]
    weights, own_w = (UP, DN), (up_in, dn_in)

    def region(ref, start, ph, i):
        row, col, n_col, _ = cuts[ph][i]
        row = pl.multiple_of(start + row, UNIT)
        if n_col == hid:
            return ref.at[pl.ds(row, UNIT), :]
        return ref.at[pl.ds(row, UNIT), pl.ds(pl.multiple_of(col, 128), n_col)]

    def piece(ph, origin, i):
        return region(weights[ph], origin * wrows, ph, i)

    def hop0(ph, i):
        src = region(own_w[ph], 0 * me, ph, i)
        remote(src, piece(ph, me, i), SR.at[ph, i], RR.at[ph, i, 1], sp=right).start()
        remote(src, piece(ph, me, i), SL.at[ph, i], RL.at[ph, i, 1], sp=left).start()

    def to_pair(ph, origin, i):
        if cuts[ph][i][3]:
            k = rem(lax.div(origin, jnp.int32(SUB)) - gz + ng, ng)
            part = piece(ph, origin, i)
            remote(part, part, SY.at[ph, i], RY.at[ph, i, k], grp=pair).start()

    def from_pair(ph, k):
        rows = (SUB if k else SUB - 1) * UNIT
        for i, (_, _, n_col, shared) in enumerate(cuts[ph]):
            if shared:
                drain(weights[ph].at[pl.ds(0, rows), pl.ds(0, n_col)], RY.at[ph, i, k])

    def tick(h, fill=()):
        fill = list(fill)
        slots = 2 * len(order)

        def work(n):
            for f in fill[n * len(fill) // slots : (n + 1) * len(fill) // slots]:
                f()

        from_left, from_right = rem(me - h + nz, nz), rem(me + h, nz)
        for n, (ph, i) in enumerate(order):
            a, b = piece(ph, from_left, i), piece(ph, from_right, i)
            remote(a, a, SR.at[ph, i], RR.at[ph, i, h], sp=right).wait_recv()

            @pl.when(h < n_right)
            def _():
                remote(a, a, SR.at[ph, i], RR.at[ph, i, h + 1], sp=right).start()

            to_pair(ph, from_left, i)
            work(2 * n)

            @pl.when(h <= n_left)
            def _():
                remote(b, b, SL.at[ph, i], RL.at[ph, i, h], sp=left).wait_recv()

                @pl.when(h < n_left)
                def _():
                    remote(b, b, SL.at[ph, i], RL.at[ph, i, h + 1], sp=left).start()

                to_pair(ph, from_right, i)

            work(2 * n + 1)

    def ticks(first, last):
        def body(h, _):
            tick(h)
            return 0

        lax.fori_loop(first, last + 1, body, 0)

    for ph, i in order:
        hop0(ph, i)

    waits = []

    def wo_rows(s):
        return WO.at[pl.ds(pl.multiple_of(s * dh, dh), dh), :]

    def res_rows(s):
        return RES.at[pl.ds(pl.multiple_of(s * own_rows, own_rows), own_rows), :]

    def mix_cols(s):
        return MIX.at[:, pl.ds(pl.multiple_of(s * dh, dh), dh)]

    def spread(which, own, region):
        for d in [2, 1, 3, *range(4, nx)]:
            if d < nx:
                copy = remote(own, region(t), SX.at[which, d], RX.at[which, d], tp=rem(x + d, nx) * CORES + c)
                copy.start()
                waits.append(copy)
        copy = remote(own, region(t), SD.at[which, 0], RD.at[which, 0], tp=sib)
        copy.start()
        waits.append(copy)

    def pass_on(which, region):
        for d in range(1, nx):
            part = region(rem(x - d + nx, nx) * CORES + c)
            remote(part, part, SX.at[which, d], RX.at[which, d], tp=sib).wait_recv()
            copy = remote(part, part, SD.at[which, d], RD.at[which, d], tp=sib)
            copy.start()
            waits.append(copy)

    def passed(which, region):
        for d in range(nx):
            part = region(rem(x - d + nx, nx) * CORES + 1 - c)
            remote(part, part, SD.at[which, d], RD.at[which, d], tp=sib).wait_recv()

    spread(0, res_in, res_rows)
    spread(1, wo_in, wo_rows)

    lane = lax.broadcasted_iota(jnp.int32, (1, BLOCK), 1)
    scale = dh ** (-0.5)
    total = top = memory = None
    for b in range(nb):
        cols = slice(b * BLOCK, (b + 1) * BLOCK)
        f = fg_ref[:, cols]
        cum = jnp.minimum(f, 0.0) - jnp.log1p(jnp.exp(-jnp.abs(f))) + ex_ref[:, cols]
        step = 1
        while step < BLOCK:
            cum = cum + jnp.where(lane >= step, pltpu.roll(cum, step, 1), 0.0)
            step *= 2
        ST[b : b + 1, :] = cum
        whole = jnp.sum(jnp.where(lane == BLOCK - 1, cum, 0.0), axis=1, keepdims=True)
        tail = whole - cum + ig_ref[:, cols]
        tail_top = jnp.max(tail, axis=1, keepdims=True)
        weight = jnp.exp(tail - tail_top)
        keys_t = k_ref[cols, :].astype(F32).T
        part = two_part_dot(keys_t * weight, v_ref[cols, :]) * scale
        if b == 0:
            total, top, memory = whole, tail_top, part
        else:
            LM[b - 1] = memory
            ST[8 + b : 9 + b, :] = jnp.broadcast_to(total, (1, BLOCK))
            ST[16 + b : 17 + b, :] = jnp.broadcast_to(top, (1, BLOCK))
            new_top = jnp.maximum(whole + top, tail_top)
            memory = jnp.exp(whole + top - new_top) * memory + jnp.exp(tail_top - new_top) * part
            total, top = total + whole, new_top
    srows = dh // SUB
    for i in range(SUB):
        AS[i, 0:srows, :] = memory[i * srows : (i + 1) * srows, :]
        AS[i, srows : srows + 1, :] = jnp.broadcast_to(total, (1, dh))
        AS[i, srows + 1 : srows + 2, :] = jnp.broadcast_to(top, (1, dh))
    for d in range(1, SUB):
        i = rem(j + d, SUB)
        copy = remote(AS.at[i], AR.at[j], SA.at[d], RA.at[d], sp=gz * SUB + i)
        copy.start()
        waits.append(copy)
    AR[j] = AS[j]
    UP[pl.ds(pl.multiple_of(me * wrows, wrows), wrows), :] = up_in[...]
    DN[pl.ds(pl.multiple_of(me * wrows, wrows), wrows), :] = dn_in[...]
    WO[pl.ds(pl.multiple_of(t * dh, dh), dh), :] = wo_in[...]
    RES[pl.ds(pl.multiple_of(t * own_rows, own_rows), own_rows), :] = res_in[...]

    def member(i):
        return AR[i, 0:srows, :], AR[i, srows : srows + 1, :], AR[i, srows + 1 : srows + 2, :]

    def fold(state, top, member_state):
        part, part_total, part_top = member_state
        new_top = jnp.maximum(part_total + top, part_top)
        return jnp.exp(part_total + top - new_top) * state + jnp.exp(part_top - new_top) * part, new_top

    def group_state():
        for d in range(1, SUB):
            slot = AR.at[rem(j - d + SUB, SUB)]
            remote(slot, slot, SA.at[d], RA.at[d], sp=right).wait_recv()
        g_state, g_total, g_top = member(0)
        for i in range(1, SUB):
            m_state = member(i)
            g_state, g_top = fold(g_state, g_top, m_state)
            g_total = g_total + m_state[1]
        GX[0:srows, :] = g_state
        GX[srows : srows + 1, :] = g_total
        GX[srows + 1 : srows + 2, :] = g_top

    def chain():
        @pl.when(gz > 0)
        def _():
            remote(BR, BR, SB.at[0], RB.at[0], sp=right).wait_recv()

        @pl.when(gz == 0)
        def _():
            BR[...] = jnp.zeros_like(BR)

        state, top = BR[0:srows, :], BR[srows + 1 : srows + 2, :]
        after, after_top = fold(
            state, top, (GX[0:srows, :], GX[srows : srows + 1, :], GX[srows + 1 : srows + 2, :])
        )
        BS[0:srows, :] = after
        BS[srows + 1 : srows + 2, :] = after_top

        @pl.when(gz < ng - 1)
        def _():
            remote(BS, BR, SB.at[0], RB.at[0], sp=rem(me + SUB, nz)).start()

        for i in range(SUB):
            CS[i, 0:srows, :] = state
            CS[i, srows + 1 : srows + 2, :] = top
            if i < SUB - 1:
                state, top = fold(state, top, member(i))
        for d in range(1, SUB):
            i = rem(j + d, SUB)
            remote(CS.at[i], CR.at[j], SC.at[d], RC.at[d], sp=gz * SUB + i).start()
        CR[j] = CS[j]

    early, first = ng - CHAIN_LATE, 2

    @pl.when(gz < early)
    def _():
        group_state()
        chain()

    ticks(1, first)

    @pl.when(gz >= early)
    def _():
        group_state()

    def chain_tick(r, _):
        tick(first + 1 + r)

        @pl.when(gz == early + r)
        def _():
            chain()

        return 0

    lax.fori_loop(0, CHAIN_LATE, chain_tick, 0)
    at_tick = first + CHAIN_LATE

    def next_tick(fill=()):
        nonlocal at_tick
        if at_tick < n_right:
            at_tick += 1
            tick(at_tick, fill)
        else:
            for f in fill:
                f()

    next_tick()

    for d in range(1, SUB):
        slot = CR.at[rem(j - d + SUB, SUB)]
        remote(slot, slot, SC.at[d], RC.at[d], sp=right).wait_recv()
    before = jnp.concatenate([CR[i, 0:srows, :] for i in range(SUB)], axis=0)
    before_top = CR[0, srows + 1 : srows + 2, :]
    causal = lax.broadcasted_iota(jnp.int32, (BLOCK, BLOCK), 0) >= lax.broadcasted_iota(
        jnp.int32, (BLOCK, BLOCK), 1
    )
    mine = pl.ds(pl.multiple_of(t * dh, dh), dh)
    def hidden_block(b):
        cols = slice(b * BLOCK, (b + 1) * BLOCK)
        cum = ST[b : b + 1, :]
        if b == 0:
            start, start_top = before, before_top
        else:
            total, top = ST[8 + b : 9 + b, :], ST[16 + b : 17 + b, :]
            start_top = jnp.maximum(total + before_top, top)
            start = jnp.exp(total + before_top - start_top) * before + jnp.exp(top - start_top) * LM[b - 1]
        cum_t = jnp.broadcast_to(cum, (BLOCK, BLOCK)).T
        log_weight = jnp.where(causal, cum_t - cum + ig_ref[:, cols], NEG_BIG)
        carry_log = cum_t + start_top
        row_max = jnp.maximum(jnp.max(log_weight, axis=1, keepdims=True), carry_log)
        q, k, v = q_ref[cols, :], k_ref[cols, :], v_ref[cols, :]
        qk = lax.dot_general(q, k, (((1,), (1,)), ((), ())), preferred_element_type=F32) * scale
        hidden = two_part_dot(qk * jnp.exp(log_weight - row_max), v)
        hidden = hidden + jnp.exp(carry_log - row_max) * dot_two_part(q, start)
        mean_sq = jnp.mean(hidden * hidden, axis=1, keepdims=True)
        gate = jax.nn.sigmoid(og_ref[cols, :].astype(F32))
        mixed = hidden * lax.rsqrt(mean_sq + NORM_EPS) * hng_ref[...] * gate
        MIX[cols, mine] = mixed.astype(BF16)

    next_tick([functools.partial(hidden_block, b) for b in range(nb)])
    spread(2, mix_cols(t), mix_cols)
    next_tick()
    pass_on(0, res_rows)
    pass_on(1, wo_rows)
    pass_on(2, mix_cols)
    next_tick()
    for which, rows in ((0, res_rows), (1, wo_rows), (2, mix_cols)):
        passed(which, rows)

    SSQ[...] = jnp.zeros_like(SSQ)

    def project(n):
        at = slice(n * 256, (n + 1) * 256)
        branch = jnp.dot(MIX[...], WO[:, at], preferred_element_type=F32)
        mid = (RES[:, at].astype(F32) + branch).astype(BF16)
        MID[:, at] = mid
        wide = mid.astype(F32)
        SSQ[...] += wide[:, :128] * wide[:, :128] + wide[:, 128:] * wide[:, 128:]

    def normalize(n):
        at = slice(n * 64, (n + 1) * 64)
        mean_sq = jnp.sum(SSQ[at, :], axis=1, keepdims=True) / width
        NRM[at, :] = (MID[at, :].astype(F32) * lax.rsqrt(mean_sq + NORM_EPS) * fng_ref[...]).astype(BF16)

    n_cols = width // 256
    projects = [functools.partial(project, n) for n in range(n_cols)]
    next_tick(projects[: n_cols // 2])
    next_tick(projects[n_cols // 2 :])
    next_tick([functools.partial(normalize, n) for n in range(tok // 64)])

    def group_of(k):
        return rem(gz + k, ng)

    def upward(k, n, final):
        at = slice(n * hid_half, (n + 1) * hid_half)
        rows = pl.ds(pl.multiple_of(group_of(k) * gcols, gcols), gcols)
        value = jnp.dot(NRM[:, rows], UP[rows, at], preferred_element_type=F32)
        if k:
            value = value + UACC[:, at]
        if final:
            value = jnp.maximum(value, 0.0)
            ACT[:, at] = (value * value).astype(BF16)
        else:
            UACC[:, at] = value

    def ups(k, final=False):
        first_half = functools.partial(upward, k, 0, final)

        def start():
            if share:
                from_pair(0, k)
            first_half()

        return [start, functools.partial(upward, k, 1, final)]

    def down(k):
        if share:
            from_pair(1, k)
        rows = pl.ds(pl.multiple_of(group_of(k) * gcols, gcols), gcols)
        value = lax.dot_general(
            ACT[...], DN[rows, :], (((1,), (1,)), ((), ())), preferred_element_type=F32
        )
        PART[k] = value.astype(BF16).reshape(nx, CORES, own_rows, gcols)
        copy = remote(PART.at[k, :, 1 - c], SIB.at[k], SP.at[k], RP.at[k], tp=sib)
        copy.start()
        waits.append(copy)

    def add_up(k):
        remote(SIB.at[k], SIB.at[k], SP.at[k], RP.at[k], tp=sib).wait_recv()
        for i in range(nx):
            SUM[k, i] = (PART[k, i, c].astype(F32) + SIB[k, i].astype(F32)).astype(BF16)
        for d in [2, 1, 3, *range(4, nx)]:
            if d < nx:
                i = rem(x + d, nx)
                copy = remote(SUM.at[k, i], RSR.at[k, x], SQ.at[k, d], RQ.at[k, d], tp=i * CORES + c)
                copy.start()
                waits.append(copy)

    def finish(k):
        at = pl.ds(pl.multiple_of(group_of(k) * gcols, gcols), gcols)
        value = MID[pl.ds(pl.multiple_of(t * own_rows, own_rows), own_rows), at].astype(F32)
        value = value + SUM[k, x].astype(F32)
        for d in range(1, nx):
            slot = RSR.at[k, rem(x - d + nx, nx)]
            remote(slot, slot, SQ.at[k, d], RQ.at[k, d], tp=sib).wait_recv()
            value = value + RSR[k, rem(x - d + nx, nx)].astype(F32)
        out_ref[:, at] = value.astype(BF16)

    turn = [0]
    for n in range(1, ng // 2):
        turn += [ng - n, n]
    turn += [ng // 2]
    ready = [SUB - 1] + [SUB * (n // 2 + 1) + SUB - 1 for n in range(ng - 2)] + [n_right]
    left_up = list(turn)
    while at_tick < n_right:
        n_ready = sum(ready[turn.index(k)] <= at_tick for k in left_up[:-1])
        per = min(n_ready, -(-len(left_up[:-1]) // (n_right - at_tick)))
        fill = []
        for k in left_up[:per]:
            fill += ups(k)
        left_up = left_up[per:]
        next_tick(fill)
    for k in left_up:
        for f in ups(k, final=k == turn[-1]):
            f()
    for n, k in enumerate(turn):
        down(k)
        if n > 1:
            add_up(turn[n - 2])
        if n > 4:
            finish(turn[n - 5])
    for k in turn[-2:]:
        add_up(k)
    for k in turn[ng - 5 :]:
        finish(k)

    for ph, i in order:
        n_col, shared = cuts[ph][i][2:]
        cols = pl.ds(0, n_col)
        drain(weights[ph].at[pl.ds(0, n_right * UNIT), cols], SR.at[ph, i])
        drain(weights[ph].at[pl.ds(0, n_left * UNIT), cols], SL.at[ph, i])
        if shared:
            drain(weights[ph].at[pl.ds(0, (nz - 1) * UNIT), cols], SY.at[ph, i])
    for copy in waits:
        copy.wait_send()
    for d in range(1, SUB):
        drain(CS.at[0], SC.at[d])

    @pl.when(gz < ng - 1)
    def _():
        drain(BS, SB.at[0])


def shards(
    sizes,
    queries,
    memory_keys,
    memory_values,
    output_preactivation,
    input_preactivation,
    forget_preactivation,
    extra_forget_terms,
    head_norm_gain,
    output_projection_matrix,
    residual,
    feedforward_norm_gain,
    feedforward_up_matrix,
    feedforward_down_matrix,
):
    nz, nt, share = sizes
    nx, ng = nt // CORES, nz // SUB
    tok, dh = queries.shape
    own_rows, width = residual.shape
    wrows, hid = feedforward_up_matrix.shape
    n_right = nz // 2
    n_pieces = 3 if share else 4
    gcols = SUB * wrows
    msg = (dh // SUB + 8, dh)
    dma = pltpu.SemaphoreType.DMA
    vmem = pltpu.VMEM
    scratch = [
        vmem((nz * wrows, hid), BF16),
        vmem((nz * wrows, hid), BF16),
        vmem((nt * dh, width), BF16),
        vmem((tok, width), BF16),
        vmem((tok, nt * dh), BF16),
        vmem((tok, width), BF16),
        vmem((tok, width), BF16),
        vmem((tok, 128), F32),
        vmem((tok, hid), F32),
        vmem((tok, hid), BF16),
        vmem((ng, nx, CORES, own_rows, gcols), BF16),
        vmem((ng, nx, own_rows, gcols), BF16),
        vmem((ng, nx, own_rows, gcols), BF16),
        vmem((ng, nx, own_rows, gcols), BF16),
        vmem((tok // BLOCK - 1, dh, dh), F32),
        vmem((24, BLOCK), F32),
        vmem((SUB, *msg), F32),
        vmem((SUB, *msg), F32),
        vmem(msg, F32),
        vmem(msg, F32),
        vmem(msg, F32),
        vmem((SUB, *msg), F32),
        vmem((SUB, *msg), F32),
        dma((2, n_pieces)),
        dma((2, n_pieces, n_right + 1)),
        dma((2, n_pieces)),
        dma((2, n_pieces, n_right + 1)),
        dma((2, n_pieces)),
        dma((2, n_pieces, ng)),
        dma((3, nx)),
        dma((3, nx)),
        dma((3, nx)),
        dma((3, nx)),
        dma((SUB,)),
        dma((SUB,)),
        dma((1,)),
        dma((1,)),
        dma((SUB,)),
        dma((SUB,)),
        dma((ng,)),
        dma((ng,)),
        dma((ng, nx)),
        dma((ng, nx)),
    ]
    return pl.pallas_call(
        functools.partial(kernel, sizes),
        out_shape=jax.ShapeDtypeStruct((own_rows, width), BF16),
        in_specs=[pl.BlockSpec(memory_space=pltpu.VMEM)] * 13,
        out_specs=pl.BlockSpec(memory_space=pltpu.VMEM),
        scratch_shapes=scratch,
        compiler_params=pltpu.CompilerParams(
            collective_id=0, has_side_effects=True, vmem_limit_bytes=56 * 1024 * 1024
        ),
        name="layer",
    )(
        queries,
        memory_keys,
        memory_values,
        output_preactivation,
        input_preactivation,
        forget_preactivation,
        extra_forget_terms,
        head_norm_gain.reshape(1, -1),
        output_projection_matrix,
        residual,
        feedforward_norm_gain.reshape(1, -1),
        feedforward_up_matrix,
        feedforward_down_matrix.T,
    )


def solution(mesh):
    in_specs = (
        P(("grp", "sp"), "tp"),
        P(("grp", "sp"), "tp"),
        P(("grp", "sp"), "tp"),
        P(("grp", "sp"), "tp"),
        P("tp", ("grp", "sp")),
        P("tp", ("grp", "sp")),
        P("tp", ("grp", "sp")),
        P(),
        P("tp", None),
        P(("grp", "sp", "tp"), None),
        P(),
        P("sp", "tp"),
        P("tp", "sp"),
    )
    out_specs = P(("grp", "sp", "tp"), None)
    sizes = (mesh.shape["sp"], mesh.shape["tp"], mesh.shape["grp"] % 2 == 0)
    return jax.shard_map(
        functools.partial(shards, sizes), mesh=mesh, in_specs=in_specs, out_specs=out_specs, check_vma=False
    )
```

```python
import functools

import jax
import jax.numpy as jnp
from jax import lax
from jax.experimental import pallas as pl
from jax.experimental.pallas import tpu as pltpu
from jax.sharding import PartitionSpec as P

BLOCK = 128
CHAIN_LATE = 5
CORES = 2
SUB = 4
UNIT = 16
NORM_EPS = 1e-06
NEG_BIG = -1e30
MESH = pl.DeviceIdType.MESH
F32 = jnp.float32
BF16 = jnp.bfloat16


def two_part_dot(a, b, dims=(((1,), (0,)), ((), ()))):
    high = a.astype(BF16)
    low = (a - high.astype(F32)).astype(BF16)
    dot = functools.partial(lax.dot_general, dimension_numbers=dims, preferred_element_type=F32)
    return dot(high, b) + dot(low, b)


def dot_two_part(a, b):
    high = b.astype(BF16)
    low = (b - high.astype(F32)).astype(BF16)
    return jnp.dot(a, high, preferred_element_type=F32) + jnp.dot(a, low, preferred_element_type=F32)


def rem(a, b):
    return lax.rem(a, jnp.int32(b))


def kernel(
    sizes,
    q_ref, k_ref, v_ref, og_ref, ig_ref, fg_ref, ex_ref, hng_ref, wo_in, res_in, fng_ref, up_in, dn_in,
    out_ref,
    UP, DN, WO, RES, OWN, MIX, MID, NRM, SSQ, UACC, ACT, PART, SIB, SUM, RSR, LM, ST, AS, AR, GX, BS, BR, CS, CR,
    SR, RR, SL, RL, SY, RY, SX, RX, SD, RD, SN, RN, SA, RA, SB, RB, SC, RC, SP, RP, SQ, RQ, WRAP,
):
    nz, nt, share = sizes
    nx = nt // CORES
    ng = nz // SUB
    n_right, n_left = nz // 2, nz - 1 - nz // 2
    tok, dh = q_ref.shape
    nb = tok // BLOCK
    width = res_in.shape[1]
    own_rows = res_in.shape[0]
    wrows, hid = up_in.shape
    gcols = SUB * wrows

    me, t, grp = lax.axis_index("sp"), lax.axis_index("tp"), lax.axis_index("grp")
    x, c = lax.div(t, jnp.int32(CORES)), rem(t, CORES)
    sib = x * CORES + 1 - c
    parity = rem(grp, 2)
    pair = grp + 1 - 2 * parity
    right, left = rem(me + 1, nz), rem(me + nz - 1, nz)
    gz, j = lax.div(me, jnp.int32(SUB)), rem(me, SUB)

    def remote(src, dst, send, recv, **device):
        return pltpu.make_async_remote_copy(
            src_ref=src, dst_ref=dst, send_sem=send, recv_sem=recv, device_id=device, device_id_type=MESH
        )

    def drain(ref, sem):
        pltpu.make_async_copy(ref, ref, sem).wait()

    barrier = pltpu.get_barrier_semaphore()

    def greet(**device):
        pl.semaphore_signal(barrier, inc=1, device_id=device, device_id_type=MESH)

    around_here = [dict(sp=gz * SUB + rem(j + d, SUB)) for d in range(1, SUB)]
    around_here += [dict(tp=rem(x + d, nx) * CORES + c) for d in range(1, nx)]
    around_here += [dict(tp=rem(x + d, nx) * CORES + 1 - c) for d in range(nx)]
    if share:
        around_here += [dict(grp=pair)]
    for device in around_here:
        greet(**device)
    greet(sp=left)

    @pl.when(me < nz - 1)
    def _():
        greet(sp=right)

    @pl.when(gz < ng - 1)
    def _():
        greet(sp=me + SUB)

    @pl.when(gz > 0)
    def _():
        greet(sp=me - SUB)

    lane = lax.broadcasted_iota(jnp.int32, (1, BLOCK), 1)
    scale = dh ** (-0.5)
    total = top = memory = None
    for b in range(nb):
        cols = slice(b * BLOCK, (b + 1) * BLOCK)
        f = fg_ref[:, cols]
        cum = jnp.minimum(f, 0.0) - jnp.log1p(jnp.exp(-jnp.abs(f))) + ex_ref[:, cols]
        step = 1
        while step < BLOCK:
            cum = cum + jnp.where(lane >= step, pltpu.roll(cum, step, 1), 0.0)
            step *= 2
        ST[b : b + 1, :] = cum
        whole = jnp.sum(jnp.where(lane == BLOCK - 1, cum, 0.0), axis=1, keepdims=True)
        tail = whole - cum + ig_ref[:, cols]
        tail_top = jnp.max(tail, axis=1, keepdims=True)
        weight = jnp.exp(tail - tail_top)
        keys_t = k_ref[cols, :].astype(F32).T
        part = two_part_dot(keys_t * weight, v_ref[cols, :]) * scale
        if b == 0:
            total, top, memory = whole, tail_top, part
        else:
            LM[b - 1] = memory
            ST[8 + b : 9 + b, :] = jnp.broadcast_to(total, (1, BLOCK))
            ST[16 + b : 17 + b, :] = jnp.broadcast_to(top, (1, BLOCK))
            new_top = jnp.maximum(whole + top, tail_top)
            memory = jnp.exp(whole + top - new_top) * memory + jnp.exp(tail_top - new_top) * part
            total, top = total + whole, new_top
    srows = dh // SUB
    for i in range(SUB):
        AS[i, 0:srows, :] = memory[i * srows : (i + 1) * srows, :]
        AS[i, srows : srows + 1, :] = jnp.broadcast_to(total, (1, dh))
        AS[i, srows + 1 : srows + 2, :] = jnp.broadcast_to(top, (1, dh))
    pl.semaphore_wait(
        barrier, len(around_here) + 1 + lax.min(me, 1) + lax.min(ng - 1 - gz, 1) + lax.min(gz, 1)
    )

    @pl.when(me == nz - 1)
    def _():
        pl.semaphore_signal(WRAP, inc=1, device_id=dict(sp=right), device_id_type=MESH)

    waits = []
    for d in range(1, SUB):
        i = rem(j + d, SUB)
        copy = remote(AS.at[i], AR.at[j], SA.at[d], RA.at[d], sp=gz * SUB + i)
        copy.start()
        waits.append(copy)
    AR[j] = AS[j]

    hid_half = hid // 2
    if share:
        mine_row, mine_col = parity * UNIT, parity * hid_half
        cuts = (
            [(3 * UNIT, 0, hid, False), (2 * UNIT, mine_col, hid_half, True), (mine_row, 0, hid, True)],
            [(2 * UNIT, 0, hid, False), (3 * UNIT, 0, hid, False), (mine_row, 0, hid, True)],
        )
        order = [(0, 2), (1, 2), (0, 1), (1, 1), (0, 0), (1, 0)]
    else:
        cuts = ([(i * UNIT, 0, hid, False) for i in range(4)],) * 2
        order = [(ph, i) for i in range(4) for ph in range(2)]
    weights, own_w = (UP, DN), (up_in, dn_in)

    def region(ref, start, ph, i):
        row, col, n_col, _ = cuts[ph][i]
        row = pl.multiple_of(start + row, UNIT)
        if n_col == hid:
            return ref.at[pl.ds(row, UNIT), :]
        return ref.at[pl.ds(row, UNIT), pl.ds(pl.multiple_of(col, 128), n_col)]

    def piece(ph, origin, i):
        return region(weights[ph], origin * wrows, ph, i)

    def hop0(to_right):
        for ph, i in order:
            src = region(own_w[ph], 0 * me, ph, i)
            if to_right:
                remote(src, piece(ph, me, i), SR.at[ph, i], RR.at[ph, i, 1], sp=right).start()
            else:
                remote(src, piece(ph, me, i), SL.at[ph, i], RL.at[ph, i, 1], sp=left).start()

    def to_pair(ph, origin, i):
        if cuts[ph][i][3]:
            k = rem(lax.div(origin, jnp.int32(SUB)) - gz + ng, ng)
            part = piece(ph, origin, i)
            remote(part, part, SY.at[ph, i], RY.at[ph, i, k], grp=pair).start()

    def from_pair(ph, k):
        rows = (SUB if k else SUB - 1) * UNIT
        for i, (_, _, n_col, shared) in enumerate(cuts[ph]):
            if shared:
                drain(weights[ph].at[pl.ds(0, rows), pl.ds(0, n_col)], RY.at[ph, i, k])

    def tick(h, fill=()):
        fill = list(fill)
        slots = 2 * len(order)

        def work(n):
            for f in fill[n * len(fill) // slots : (n + 1) * len(fill) // slots]:
                f()

        from_left, from_right = rem(me - h + nz, nz), rem(me + h, nz)
        for n, (ph, i) in enumerate(order):
            a, b = piece(ph, from_left, i), piece(ph, from_right, i)
            remote(a, a, SR.at[ph, i], RR.at[ph, i, h], sp=right).wait_recv()

            @pl.when(h < n_right)
            def _():
                remote(a, a, SR.at[ph, i], RR.at[ph, i, h + 1], sp=right).start()

            to_pair(ph, from_left, i)
            work(2 * n)

            @pl.when(h <= n_left)
            def _():
                remote(b, b, SL.at[ph, i], RL.at[ph, i, h], sp=left).wait_recv()

                @pl.when(h < n_left)
                def _():
                    remote(b, b, SL.at[ph, i], RL.at[ph, i, h + 1], sp=left).start()

                to_pair(ph, from_right, i)

            work(2 * n + 1)

    def ticks(first, last):
        def body(h, _):
            tick(h)
            return 0

        lax.fori_loop(first, last + 1, body, 0)

    hop0(True)

    @pl.when(me > 0)
    def _():
        hop0(False)


    def wo_rows(s):
        return WO.at[pl.ds(pl.multiple_of(s * dh, dh), dh), :]

    def res_rows(s):
        return RES.at[pl.ds(pl.multiple_of(s * own_rows, own_rows), own_rows), :]

    def mix_cols(s):
        return pl.ds(pl.multiple_of(s * dh, dh), dh)

    def around(d):
        return rem(x + d, nx), rem(x - d + nx, nx)

    hops = [d for d in [2, 1, 3, *range(4, nx)] if d < nx]

    def begin(*args, **device):
        copy = remote(*args, **device)
        copy.start()
        waits.append(copy)

    for d in hops:
        begin(res_in, res_rows(x), SX.at[0, d], RX.at[0, d], tp=around(d)[0] * CORES + c)
    for d in hops:
        begin(wo_in, wo_rows(t), SX.at[1, d], RX.at[1, d], tp=around(d)[0] * CORES + c)
    begin(wo_in, wo_rows(t), SD.at[1, 0], RD.at[1, 0], tp=sib)

    def pass_on():
        for d in hops:
            part = wo_rows(around(d)[1] * CORES + c)
            remote(part, part, SX.at[1, d], RX.at[1, d], tp=sib).wait_recv()
            begin(part, part, SD.at[1, d], RD.at[1, d], tp=sib)

    def project_ready():
        for d in hops:
            part = res_rows(around(d)[1])
            remote(part, part, SX.at[0, d], RX.at[0, d], tp=sib).wait_recv()
        for d in range(nx):
            part = wo_rows(around(d)[1] * CORES + 1 - c)
            remote(part, part, SD.at[1, d], RD.at[1, d], tp=sib).wait_recv()
        for d in range(nx):
            here = around(d)[1] * CORES
            if d:
                drain(MIX.at[:, mix_cols(here + c)], RX.at[2, d])
            drain(MIX.at[:, mix_cols(here + 1 - c)], RD.at[2, d])

    UP[pl.ds(pl.multiple_of(me * wrows, wrows), wrows), :] = up_in[...]
    DN[pl.ds(pl.multiple_of(me * wrows, wrows), wrows), :] = dn_in[...]
    WO[pl.ds(pl.multiple_of(t * dh, dh), dh), :] = wo_in[...]
    RES[pl.ds(pl.multiple_of(x * own_rows, own_rows), own_rows), :] = res_in[...]

    def member(i):
        return AR[i, 0:srows, :], AR[i, srows : srows + 1, :], AR[i, srows + 1 : srows + 2, :]

    def fold(state, top, member_state):
        part, part_total, part_top = member_state
        new_top = jnp.maximum(part_total + top, part_top)
        return jnp.exp(part_total + top - new_top) * state + jnp.exp(part_top - new_top) * part, new_top

    def group_state():
        for d in range(1, SUB):
            slot = AR.at[rem(j - d + SUB, SUB)]
            remote(slot, slot, SA.at[d], RA.at[d], sp=right).wait_recv()
        g_state, g_total, g_top = member(0)
        for i in range(1, SUB):
            m_state = member(i)
            g_state, g_top = fold(g_state, g_top, m_state)
            g_total = g_total + m_state[1]
        GX[0:srows, :] = g_state
        GX[srows : srows + 1, :] = g_total
        GX[srows + 1 : srows + 2, :] = g_top

    def chain():
        @pl.when(gz > 0)
        def _():
            remote(BR, BR, SB.at[0], RB.at[0], sp=right).wait_recv()

        @pl.when(gz == 0)
        def _():
            BR[...] = jnp.zeros_like(BR)

        state, top = BR[0:srows, :], BR[srows + 1 : srows + 2, :]
        after, after_top = fold(
            state, top, (GX[0:srows, :], GX[srows : srows + 1, :], GX[srows + 1 : srows + 2, :])
        )
        BS[0:srows, :] = after
        BS[srows + 1 : srows + 2, :] = after_top

        @pl.when(gz < ng - 1)
        def _():
            remote(BS, BR, SB.at[0], RB.at[0], sp=rem(me + SUB, nz)).start()

        for i in range(SUB):
            CS[i, 0:srows, :] = state
            CS[i, srows + 1 : srows + 2, :] = top
            if i < SUB - 1:
                state, top = fold(state, top, member(i))
        for d in range(1, SUB):
            i = rem(j + d, SUB)
            remote(CS.at[i], CR.at[j], SC.at[d], RC.at[d], sp=gz * SUB + i).start()
        CR[j] = CS[j]

    early = ng - CHAIN_LATE

    @pl.when(gz < early)
    def _():
        group_state()
        chain()

    @pl.when(me == 0)
    def _():
        pl.semaphore_wait(WRAP, 1)
        hop0(False)

    at_tick = 0

    def next_tick(fill=()):
        nonlocal at_tick
        if at_tick < n_right:
            at_tick += 1
            tick(at_tick, fill)
        else:
            for f in fill:
                f()

    def nothing():
        pass

    def chain_at(g):
        @pl.when(gz == g)
        def _():
            chain()

    next_tick()

    @pl.when(gz >= early)
    def _():
        group_state()

    chain_at(early)
    for g in range(early + 1, ng, 2):
        next_tick()
        next_tick([functools.partial(chain_at, g), nothing])
        if g + 1 < ng:
            next_tick()
            chain_at(g + 1)

    def state_before():
        for d in range(1, SUB):
            slot = CR.at[rem(j - d + SUB, SUB)]
            remote(slot, slot, SC.at[d], RC.at[d], sp=right).wait_recv()

    causal = lax.broadcasted_iota(jnp.int32, (BLOCK, BLOCK), 0) >= lax.broadcasted_iota(
        jnp.int32, (BLOCK, BLOCK), 1
    )
    def hidden_block(b):
        before = jnp.concatenate([CR[i, 0:srows, :] for i in range(SUB)], axis=0)
        before_top = CR[0, srows + 1 : srows + 2, :]
        cols = slice(b * BLOCK, (b + 1) * BLOCK)
        cum = ST[b : b + 1, :]
        if b == 0:
            start, start_top = before, before_top
        else:
            total, top = ST[8 + b : 9 + b, :], ST[16 + b : 17 + b, :]
            start_top = jnp.maximum(total + before_top, top)
            start = jnp.exp(total + before_top - start_top) * before + jnp.exp(top - start_top) * LM[b - 1]
        cum_t = jnp.broadcast_to(cum, (BLOCK, BLOCK)).T
        log_weight = jnp.where(causal, cum_t - cum + ig_ref[:, cols], NEG_BIG)
        carry_log = cum_t + start_top
        row_max = jnp.maximum(jnp.max(log_weight, axis=1, keepdims=True), carry_log)
        q, k, v = q_ref[cols, :], k_ref[cols, :], v_ref[cols, :]
        qk = lax.dot_general(q, k, (((1,), (1,)), ((), ())), preferred_element_type=F32) * scale
        hidden = two_part_dot(qk * jnp.exp(log_weight - row_max), v)
        hidden = hidden + jnp.exp(carry_log - row_max) * dot_two_part(q, start)
        mean_sq = jnp.mean(hidden * hidden, axis=1, keepdims=True)
        gate = jax.nn.sigmoid(og_ref[cols, :].astype(F32))
        mixed = hidden * lax.rsqrt(mean_sq + NORM_EPS) * hng_ref[...] * gate
        mixed = mixed.astype(BF16)
        half = slice(b * own_rows, (b + 1) * own_rows)
        for core in range(CORES):
            OWN[core, half, :] = mixed[core * own_rows : (core + 1) * own_rows, :]
        MIX[half, mix_cols(t)] = OWN[c, half, :]
        for d in [*hops, 0]:
            there = around(d)[0] * CORES
            dst = MIX.at[half, mix_cols(t)]
            if d:
                remote(OWN.at[c, half], dst, SX.at[2, d], RX.at[2, d], tp=there + c).start()
            remote(OWN.at[1 - c, half], dst, SD.at[2, d], RD.at[2, d], tp=there + 1 - c).start()

    blocks = [functools.partial(hidden_block, b) for b in range(nb)]
    next_tick()
    next_tick([nothing, state_before, blocks[0]])
    next_tick(blocks[1:])
    next_tick([pass_on, nothing])
    next_tick([nothing, project_ready])

    SSQ[...] = jnp.zeros_like(SSQ)

    def project(n):
        at = slice(n * 256, (n + 1) * 256)
        branch = jnp.dot(MIX[...], WO[:, at], preferred_element_type=F32)
        mid = (RES[:, at].astype(F32) + branch).astype(BF16)
        MID[:, at] = mid
        wide = mid.astype(F32)
        SSQ[...] += wide[:, :128] * wide[:, :128] + wide[:, 128:] * wide[:, 128:]

    def normalize(n):
        at = slice(n * own_rows, (n + 1) * own_rows)
        rows = pl.ds(pl.multiple_of((n * CORES + c) * own_rows, own_rows), own_rows)
        mean_sq = jnp.sum(SSQ[at, :], axis=1, keepdims=True) / width
        NRM[rows, :] = (MID[at, :].astype(F32) * lax.rsqrt(mean_sq + NORM_EPS) * fng_ref[...]).astype(BF16)
        begin(NRM.at[rows, :], NRM.at[rows, :], SN.at[n], RN.at[n], tp=sib)

    def normed_ready():
        for n in range(nx):
            rows = pl.ds(pl.multiple_of((n * CORES + 1 - c) * own_rows, own_rows), own_rows)
            remote(NRM.at[rows, :], NRM.at[rows, :], SN.at[n], RN.at[n], tp=sib).wait_recv()

    n_cols = width // 256
    next_tick([functools.partial(project, n) for n in range(n_cols // 2)])
    next_tick([functools.partial(project, n) for n in range(n_cols // 2, n_cols)])
    next_tick([functools.partial(normalize, n) for n in range(nx)])
    normed_ready()

    def group_of(k):
        return rem(gz + k, ng)

    turn = [0]
    for n in range(1, ng // 2):
        turn += [ng - n, n]
    turn += [ng // 2]

    def upward(ks, n, n_col, final):
        at = slice(n * n_col, (n + 1) * n_col)
        value = None
        for k in ks:
            rows = pl.ds(pl.multiple_of(group_of(k) * gcols, gcols), gcols)
            part = jnp.dot(NRM[:, rows], UP[rows, at], preferred_element_type=F32)
            value = part if value is None else value + part
        if final:
            value = jnp.maximum(value + UACC[:, at], 0.0)
            ACT[:, at] = (value * value).astype(BF16)
        else:
            UACC[:, at] = value

    near = 2 * ((n_right - SUB) // SUB) - 1
    if share:
        for k in turn[:near]:
            from_pair(0, k)
    next_tick([functools.partial(upward, turn[:near], n, 128, False) for n in range(hid // 128)])
    if share:
        for k in turn[near:]:
            from_pair(0, k)
    for n in range(hid // 256):
        upward(turn[near:], n, 256, True)

    def down(k):
        if share:
            from_pair(1, k)
        rows = pl.ds(pl.multiple_of(group_of(k) * gcols, gcols), gcols)
        value = lax.dot_general(
            ACT[...], DN[rows, :], (((1,), (1,)), ((), ())), preferred_element_type=F32
        )
        PART[k] = value.astype(BF16).reshape(nx, CORES, own_rows, gcols)
        copy = remote(PART.at[k, :, 1 - c], SIB.at[k], SP.at[k], RP.at[k], tp=sib)
        copy.start()
        waits.append(copy)

    def add_up(k):
        remote(SIB.at[k], SIB.at[k], SP.at[k], RP.at[k], tp=sib).wait_recv()
        for i in range(nx):
            SUM[k, i] = (PART[k, i, c].astype(F32) + SIB[k, i].astype(F32)).astype(BF16)
        for d in [2, 1, 3, *range(4, nx)]:
            if d < nx:
                i = rem(x + d, nx)
                copy = remote(SUM.at[k, i], RSR.at[k, x], SQ.at[k, d], RQ.at[k, d], tp=i * CORES + c)
                copy.start()
                waits.append(copy)

    def finish(k):
        at = pl.ds(pl.multiple_of(group_of(k) * gcols, gcols), gcols)
        value = MID[pl.ds(pl.multiple_of(x * own_rows, own_rows), own_rows), at].astype(F32)
        value = value + SUM[k, x].astype(F32)
        for d in range(1, nx):
            slot = RSR.at[k, rem(x - d + nx, nx)]
            remote(slot, slot, SQ.at[k, d], RQ.at[k, d], tp=sib).wait_recv()
            value = value + RSR[k, rem(x - d + nx, nx)].astype(F32)
        out_ref[:, at] = value.astype(BF16)

    for n, k in enumerate(turn):
        down(k)
        if n > 1:
            add_up(turn[n - 2])
        if n > 4:
            finish(turn[n - 5])
    for k in turn[-2:]:
        add_up(k)
    for k in turn[ng - 5 :]:
        finish(k)

    for ph, i in order:
        n_col, shared = cuts[ph][i][2:]
        cols = pl.ds(0, n_col)
        drain(weights[ph].at[pl.ds(0, n_right * UNIT), cols], SR.at[ph, i])
        drain(weights[ph].at[pl.ds(0, n_left * UNIT), cols], SL.at[ph, i])
        if shared:
            drain(weights[ph].at[pl.ds(0, (nz - 1) * UNIT), cols], SY.at[ph, i])
    for copy in waits:
        copy.wait_send()
    for d in range(1, SUB):
        drain(CS.at[0], SC.at[d])
    for d in range(nx):
        if d:
            drain(OWN.at[0], SX.at[2, d])
        drain(OWN.at[0], SD.at[2, d])

    @pl.when(gz < ng - 1)
    def _():
        drain(BS, SB.at[0])


def shards(
    sizes,
    queries,
    memory_keys,
    memory_values,
    output_preactivation,
    input_preactivation,
    forget_preactivation,
    extra_forget_terms,
    head_norm_gain,
    output_projection_matrix,
    residual,
    feedforward_norm_gain,
    feedforward_up_matrix,
    feedforward_down_matrix,
):
    nz, nt, share = sizes
    nx, ng = nt // CORES, nz // SUB
    tok, dh = queries.shape
    own_rows, width = residual.shape
    wrows, hid = feedforward_up_matrix.shape
    n_right = nz // 2
    n_pieces = 3 if share else 4
    gcols = SUB * wrows
    msg = (dh // SUB + 8, dh)
    dma = pltpu.SemaphoreType.DMA
    vmem = pltpu.VMEM
    scratch = [
        vmem((nz * wrows, hid), BF16),
        vmem((nz * wrows, hid), BF16),
        vmem((nt * dh, width), BF16),
        vmem((nx * own_rows, width), BF16),
        vmem((CORES, nx * own_rows, dh), BF16),
        vmem((nx * own_rows, nt * dh), BF16),
        vmem((nx * own_rows, width), BF16),
        vmem((tok, width), BF16),
        vmem((nx * own_rows, 128), F32),
        vmem((tok, hid), F32),
        vmem((tok, hid), BF16),
        vmem((ng, nx, CORES, own_rows, gcols), BF16),
        vmem((ng, nx, own_rows, gcols), BF16),
        vmem((ng, nx, own_rows, gcols), BF16),
        vmem((ng, nx, own_rows, gcols), BF16),
        vmem((tok // BLOCK - 1, dh, dh), F32),
        vmem((24, BLOCK), F32),
        vmem((SUB, *msg), F32),
        vmem((SUB, *msg), F32),
        vmem(msg, F32),
        vmem(msg, F32),
        vmem(msg, F32),
        vmem((SUB, *msg), F32),
        vmem((SUB, *msg), F32),
        dma((2, n_pieces)),
        dma((2, n_pieces, n_right + 1)),
        dma((2, n_pieces)),
        dma((2, n_pieces, n_right + 1)),
        dma((2, n_pieces)),
        dma((2, n_pieces, ng)),
        dma((3, nx)),
        dma((3, nx)),
        dma((3, nx)),
        dma((3, nx)),
        dma((nx,)),
        dma((nx,)),
        dma((SUB,)),
        dma((SUB,)),
        dma((1,)),
        dma((1,)),
        dma((SUB,)),
        dma((SUB,)),
        dma((ng,)),
        dma((ng,)),
        dma((ng, nx)),
        dma((ng, nx)),
        pltpu.SemaphoreType.REGULAR,
    ]
    return pl.pallas_call(
        functools.partial(kernel, sizes),
        out_shape=jax.ShapeDtypeStruct((own_rows, width), BF16),
        in_specs=[pl.BlockSpec(memory_space=pltpu.VMEM)] * 13,
        out_specs=pl.BlockSpec(memory_space=pltpu.VMEM),
        scratch_shapes=scratch,
        compiler_params=pltpu.CompilerParams(
            collective_id=0, has_side_effects=True, vmem_limit_bytes=56 * 1024 * 1024
        ),
        name="layer",
    )(
        queries,
        memory_keys,
        memory_values,
        output_preactivation,
        input_preactivation,
        forget_preactivation,
        extra_forget_terms,
        head_norm_gain.reshape(1, -1),
        output_projection_matrix,
        residual,
        feedforward_norm_gain.reshape(1, -1),
        feedforward_up_matrix,
        feedforward_down_matrix.T,
    )


def solution(mesh):
    in_specs = (
        P(("grp", "sp"), "tp"),
        P(("grp", "sp"), "tp"),
        P(("grp", "sp"), "tp"),
        P(("grp", "sp"), "tp"),
        P("tp", ("grp", "sp")),
        P("tp", ("grp", "sp")),
        P("tp", ("grp", "sp")),
        P(),
        P("tp", None),
        P(("grp", "sp", "tp"), None),
        P(),
        P("sp", "tp"),
        P("tp", "sp"),
    )
    out_specs = P(("grp", "sp", "tp"), None)
    sizes = (mesh.shape["sp"], mesh.shape["tp"], mesh.shape["grp"] % 2 == 0)
    return jax.shard_map(
        functools.partial(shards, sizes), mesh=mesh, in_specs=in_specs, out_specs=out_specs, check_vma=False
    )
```

```python
import functools

import jax
import jax.numpy as jnp
from jax import lax
from jax.experimental import pallas as pl
from jax.experimental.pallas import tpu as pltpu
from jax.sharding import PartitionSpec as P

BLOCK = 128
CHAIN_LATE = 5
CORES = 2
SUB = 4
UNIT = 16
NORM_EPS = 1e-06
NEG_BIG = -1e30
MESH = pl.DeviceIdType.MESH
F32 = jnp.float32
BF16 = jnp.bfloat16


def two_part_dot(a, b, dims=(((1,), (0,)), ((), ()))):
    high = a.astype(BF16)
    low = (a - high.astype(F32)).astype(BF16)
    dot = functools.partial(lax.dot_general, dimension_numbers=dims, preferred_element_type=F32)
    return dot(high, b) + dot(low, b)


def dot_two_part(a, b):
    high = b.astype(BF16)
    low = (b - high.astype(F32)).astype(BF16)
    return jnp.dot(a, high, preferred_element_type=F32) + jnp.dot(a, low, preferred_element_type=F32)


def rem(a, b):
    return lax.rem(a, jnp.int32(b))


def kernel(
    sizes,
    q_ref, k_ref, v_ref, og_ref, ig_ref, fg_ref, ex_ref, hng_ref, wo_in, res_in, fng_ref, up_in, dn_in,
    out_ref,
    UP, DN, WO, RES, OWN, MIX, MID, NRM, SSQ, UACC, ACT, PART, SIB, SUM, RSR, LM, ST, AS, AR, GX, BS, BR, CS, CR,
    SR, RR, SL, RL, SY, RY, SX, RX, SD, RD, SN, RN, SA, RA, SB, RB, SC, RC, SP, RP, SQ, RQ, WRAP,
):
    nz, nt, share = sizes
    nx = nt // CORES
    ng = nz // SUB
    n_right, n_left = nz // 2, nz - 1 - nz // 2
    tok, dh = q_ref.shape
    nb = tok // BLOCK
    width = res_in.shape[1]
    own_rows = res_in.shape[0]
    wrows, hid = up_in.shape
    gcols = SUB * wrows

    me, t, grp = lax.axis_index("sp"), lax.axis_index("tp"), lax.axis_index("grp")
    x, c = lax.div(t, jnp.int32(CORES)), rem(t, CORES)
    sib = x * CORES + 1 - c
    parity = rem(grp, 2)
    pair = grp + 1 - 2 * parity
    right, left = rem(me + 1, nz), rem(me + nz - 1, nz)
    gz, j = lax.div(me, jnp.int32(SUB)), rem(me, SUB)

    def remote(src, dst, send, recv, **device):
        return pltpu.make_async_remote_copy(
            src_ref=src, dst_ref=dst, send_sem=send, recv_sem=recv, device_id=device, device_id_type=MESH
        )

    def drain(ref, sem):
        pltpu.make_async_copy(ref, ref, sem).wait()

    barrier = pltpu.get_barrier_semaphore()

    def greet(**device):
        pl.semaphore_signal(barrier, inc=1, device_id=device, device_id_type=MESH)

    around_here = [dict(sp=gz * SUB + rem(j + d, SUB)) for d in range(1, SUB)]
    around_here += [dict(tp=rem(x + d, nx) * CORES + c) for d in range(1, nx)]
    around_here += [dict(tp=rem(x + d, nx) * CORES + 1 - c) for d in range(nx)]
    if share:
        around_here += [dict(grp=pair)]
    for device in around_here:
        greet(**device)
    greet(sp=left)

    @pl.when(me < nz - 1)
    def _():
        greet(sp=right)

    @pl.when(gz < ng - 1)
    def _():
        greet(sp=me + SUB)

    @pl.when(gz > 0)
    def _():
        greet(sp=me - SUB)

    lane = lax.broadcasted_iota(jnp.int32, (1, BLOCK), 1)
    scale = dh ** (-0.5)
    total = top = memory = None
    for b in range(nb):
        cols = slice(b * BLOCK, (b + 1) * BLOCK)
        f = fg_ref[:, cols]
        cum = jnp.minimum(f, 0.0) - jnp.log1p(jnp.exp(-jnp.abs(f))) + ex_ref[:, cols]
        step = 1
        while step < BLOCK:
            cum = cum + jnp.where(lane >= step, pltpu.roll(cum, step, 1), 0.0)
            step *= 2
        ST[b : b + 1, :] = cum
        whole = jnp.sum(jnp.where(lane == BLOCK - 1, cum, 0.0), axis=1, keepdims=True)
        tail = whole - cum + ig_ref[:, cols]
        tail_top = jnp.max(tail, axis=1, keepdims=True)
        weight = jnp.exp(tail - tail_top)
        keys_t = k_ref[cols, :].astype(F32).T
        part = two_part_dot(keys_t * weight, v_ref[cols, :]) * scale
        if b == 0:
            total, top, memory = whole, tail_top, part
        else:
            LM[b - 1] = memory
            ST[8 + b : 9 + b, :] = jnp.broadcast_to(total, (1, BLOCK))
            ST[16 + b : 17 + b, :] = jnp.broadcast_to(top, (1, BLOCK))
            new_top = jnp.maximum(whole + top, tail_top)
            memory = jnp.exp(whole + top - new_top) * memory + jnp.exp(tail_top - new_top) * part
            total, top = total + whole, new_top
    srows = dh // SUB
    for i in range(SUB):
        AS[i, 0:srows, :] = memory[i * srows : (i + 1) * srows, :]
        AS[i, srows : srows + 1, :] = jnp.broadcast_to(total, (1, dh))
        AS[i, srows + 1 : srows + 2, :] = jnp.broadcast_to(top, (1, dh))
    pl.semaphore_wait(
        barrier, len(around_here) + 1 + lax.min(me, 1) + lax.min(ng - 1 - gz, 1) + lax.min(gz, 1)
    )

    @pl.when(me == nz - 1)
    def _():
        pl.semaphore_signal(WRAP, inc=1, device_id=dict(sp=right), device_id_type=MESH)

    waits = []
    for d in range(1, SUB):
        i = rem(j + d, SUB)
        copy = remote(AS.at[i], AR.at[j], SA.at[d], RA.at[d], sp=gz * SUB + i)
        copy.start()
        waits.append(copy)
    AR[j] = AS[j]

    hid_half = hid // 2
    if share:
        mine_row, mine_col = parity * UNIT, parity * hid_half
        cuts = (
            [(3 * UNIT, 0, hid, False), (2 * UNIT, mine_col, hid_half, True), (mine_row, 0, hid, True)],
            [(2 * UNIT, 0, hid, False), (3 * UNIT, 0, hid, False), (mine_row, 0, hid, True)],
        )
        order = [(0, 2), (1, 2), (0, 1), (1, 1), (0, 0), (1, 0)]
    else:
        cuts = ([(i * UNIT, 0, hid, False) for i in range(4)],) * 2
        order = [(ph, i) for i in range(4) for ph in range(2)]
    weights, own_w = (UP, DN), (up_in, dn_in)

    def region(ref, start, ph, i):
        row, col, n_col, _ = cuts[ph][i]
        row = pl.multiple_of(start + row, UNIT)
        if n_col == hid:
            return ref.at[pl.ds(row, UNIT), :]
        return ref.at[pl.ds(row, UNIT), pl.ds(pl.multiple_of(col, 128), n_col)]

    def piece(ph, origin, i):
        return region(weights[ph], origin * wrows, ph, i)

    def hop0(to_right):
        for ph, i in order:
            src = region(own_w[ph], 0 * me, ph, i)
            if to_right:
                remote(src, piece(ph, me, i), SR.at[ph, i], RR.at[ph, i, 1], sp=right).start()
            else:
                remote(src, piece(ph, me, i), SL.at[ph, i], RL.at[ph, i, 1], sp=left).start()

    def to_pair(ph, origin, i):
        if cuts[ph][i][3]:
            k = rem(lax.div(origin, jnp.int32(SUB)) - gz + ng, ng)
            part = piece(ph, origin, i)
            remote(part, part, SY.at[ph, i], RY.at[ph, i, k], grp=pair).start()

    def from_pair(ph, k):
        rows = (SUB if k else SUB - 1) * UNIT
        for i, (_, _, n_col, shared) in enumerate(cuts[ph]):
            if shared:
                drain(weights[ph].at[pl.ds(0, rows), pl.ds(0, n_col)], RY.at[ph, i, k])

    def tick(h, fill=()):
        fill = list(fill)
        slots = 2 * len(order)

        def work(n):
            for f in fill[n * len(fill) // slots : (n + 1) * len(fill) // slots]:
                f()

        from_left, from_right = rem(me - h + nz, nz), rem(me + h, nz)
        for n, (ph, i) in enumerate(order):
            a, b = piece(ph, from_left, i), piece(ph, from_right, i)
            remote(a, a, SR.at[ph, i], RR.at[ph, i, h], sp=right).wait_recv()

            @pl.when(h < n_right)
            def _():
                remote(a, a, SR.at[ph, i], RR.at[ph, i, h + 1], sp=right).start()

            to_pair(ph, from_left, i)
            work(2 * n)

            @pl.when(h <= n_left)
            def _():
                remote(b, b, SL.at[ph, i], RL.at[ph, i, h], sp=left).wait_recv()

                @pl.when(h < n_left)
                def _():
                    remote(b, b, SL.at[ph, i], RL.at[ph, i, h + 1], sp=left).start()

                to_pair(ph, from_right, i)

            work(2 * n + 1)

    def ticks(first, last):
        def body(h, _):
            tick(h)
            return 0

        lax.fori_loop(first, last + 1, body, 0)

    hop0(True)

    @pl.when(me > 0)
    def _():
        hop0(False)


    def wo_rows(s):
        return WO.at[pl.ds(pl.multiple_of(s * dh, dh), dh), :]

    def res_rows(s):
        return RES.at[pl.ds(pl.multiple_of(s * own_rows, own_rows), own_rows), :]

    def mix_cols(s):
        return pl.ds(pl.multiple_of(s * dh, dh), dh)

    def around(d):
        return rem(x + d, nx), rem(x - d + nx, nx)

    hops = [d for d in [2, 1, 3, *range(4, nx)] if d < nx]

    def begin(*args, **device):
        copy = remote(*args, **device)
        copy.start()
        waits.append(copy)

    for d in hops:
        begin(res_in, res_rows(x), SX.at[0, d], RX.at[0, d], tp=around(d)[0] * CORES + c)
    for d in hops:
        begin(wo_in, wo_rows(t), SX.at[1, d], RX.at[1, d], tp=around(d)[0] * CORES + c)
    begin(wo_in, wo_rows(t), SD.at[1, 0], RD.at[1, 0], tp=sib)

    def pass_on():
        for d in hops:
            part = wo_rows(around(d)[1] * CORES + c)
            remote(part, part, SX.at[1, d], RX.at[1, d], tp=sib).wait_recv()
            begin(part, part, SD.at[1, d], RD.at[1, d], tp=sib)

    def project_ready():
        for d in hops:
            part = res_rows(around(d)[1])
            remote(part, part, SX.at[0, d], RX.at[0, d], tp=sib).wait_recv()
        for d in range(nx):
            part = wo_rows(around(d)[1] * CORES + 1 - c)
            remote(part, part, SD.at[1, d], RD.at[1, d], tp=sib).wait_recv()
        for d in range(nx):
            here = around(d)[1] * CORES
            if d:
                drain(MIX.at[:, mix_cols(here + c)], RX.at[2, d])
            drain(MIX.at[:, mix_cols(here + 1 - c)], RD.at[2, d])

    UP[pl.ds(pl.multiple_of(me * wrows, wrows), wrows), :] = up_in[...]
    DN[pl.ds(pl.multiple_of(me * wrows, wrows), wrows), :] = dn_in[...]
    WO[pl.ds(pl.multiple_of(t * dh, dh), dh), :] = wo_in[...]
    RES[pl.ds(pl.multiple_of(x * own_rows, own_rows), own_rows), :] = res_in[...]

    def member(i):
        return AR[i, 0:srows, :], AR[i, srows : srows + 1, :], AR[i, srows + 1 : srows + 2, :]

    def fold(state, top, member_state):
        part, part_total, part_top = member_state
        new_top = jnp.maximum(part_total + top, part_top)
        return jnp.exp(part_total + top - new_top) * state + jnp.exp(part_top - new_top) * part, new_top

    def group_state():
        for d in range(1, SUB):
            slot = AR.at[rem(j - d + SUB, SUB)]
            remote(slot, slot, SA.at[d], RA.at[d], sp=right).wait_recv()
        g_state, g_total, g_top = member(0)
        for i in range(1, SUB):
            m_state = member(i)
            g_state, g_top = fold(g_state, g_top, m_state)
            g_total = g_total + m_state[1]
        GX[0:srows, :] = g_state
        GX[srows : srows + 1, :] = g_total
        GX[srows + 1 : srows + 2, :] = g_top

    def chain():
        @pl.when(gz > 0)
        def _():
            remote(BR, BR, SB.at[0], RB.at[0], sp=right).wait_recv()

        @pl.when(gz == 0)
        def _():
            BR[...] = jnp.zeros_like(BR)

        state, top = BR[0:srows, :], BR[srows + 1 : srows + 2, :]
        after, after_top = fold(
            state, top, (GX[0:srows, :], GX[srows : srows + 1, :], GX[srows + 1 : srows + 2, :])
        )
        BS[0:srows, :] = after
        BS[srows + 1 : srows + 2, :] = after_top

        @pl.when(gz < ng - 1)
        def _():
            remote(BS, BR, SB.at[0], RB.at[0], sp=rem(me + SUB, nz)).start()

        for i in range(SUB):
            CS[i, 0:srows, :] = state
            CS[i, srows + 1 : srows + 2, :] = top
            if i < SUB - 1:
                state, top = fold(state, top, member(i))
        for d in range(1, SUB):
            i = rem(j + d, SUB)
            remote(CS.at[i], CR.at[j], SC.at[d], RC.at[d], sp=gz * SUB + i).start()
        CR[j] = CS[j]

    early = ng - CHAIN_LATE

    @pl.when(gz < early)
    def _():
        group_state()
        chain()

    @pl.when(me == 0)
    def _():
        pl.semaphore_wait(WRAP, 1)
        hop0(False)

    at_tick = 0

    def next_tick(fill=()):
        nonlocal at_tick
        if at_tick < n_right:
            at_tick += 1
            tick(at_tick, fill)
        else:
            for f in fill:
                f()

    def nothing():
        pass

    def chain_at(g):
        @pl.when(gz == g)
        def _():
            chain()

    next_tick()

    @pl.when(gz >= early)
    def _():
        group_state()

    chain_at(early)
    for g in range(early + 1, ng, 2):
        next_tick()
        next_tick([functools.partial(chain_at, g), nothing])
        if g + 1 < ng:
            next_tick()
            chain_at(g + 1)

    def state_before():
        for d in range(1, SUB):
            slot = CR.at[rem(j - d + SUB, SUB)]
            remote(slot, slot, SC.at[d], RC.at[d], sp=right).wait_recv()

    causal = lax.broadcasted_iota(jnp.int32, (BLOCK, BLOCK), 0) >= lax.broadcasted_iota(
        jnp.int32, (BLOCK, BLOCK), 1
    )
    def hidden_block(b):
        before = jnp.concatenate([CR[i, 0:srows, :] for i in range(SUB)], axis=0)
        before_top = CR[0, srows + 1 : srows + 2, :]
        cols = slice(b * BLOCK, (b + 1) * BLOCK)
        cum = ST[b : b + 1, :]
        if b == 0:
            start, start_top = before, before_top
        else:
            total, top = ST[8 + b : 9 + b, :], ST[16 + b : 17 + b, :]
            start_top = jnp.maximum(total + before_top, top)
            start = jnp.exp(total + before_top - start_top) * before + jnp.exp(top - start_top) * LM[b - 1]
        cum_t = jnp.broadcast_to(cum, (BLOCK, BLOCK)).T
        log_weight = jnp.where(causal, cum_t - cum + ig_ref[:, cols], NEG_BIG)
        carry_log = cum_t + start_top
        row_max = jnp.maximum(jnp.max(log_weight, axis=1, keepdims=True), carry_log)
        q, k, v = q_ref[cols, :], k_ref[cols, :], v_ref[cols, :]
        qk = lax.dot_general(q, k, (((1,), (1,)), ((), ())), preferred_element_type=F32) * scale
        hidden = two_part_dot(qk * jnp.exp(log_weight - row_max), v)
        hidden = hidden + jnp.exp(carry_log - row_max) * dot_two_part(q, start)
        mean_sq = jnp.mean(hidden * hidden, axis=1, keepdims=True)
        gate = jax.nn.sigmoid(og_ref[cols, :].astype(F32))
        mixed = hidden * lax.rsqrt(mean_sq + NORM_EPS) * hng_ref[...] * gate
        mixed = mixed.astype(BF16)
        half = slice(b * own_rows, (b + 1) * own_rows)
        for core in range(CORES):
            OWN[core, half, :] = mixed[core * own_rows : (core + 1) * own_rows, :]
        MIX[half, mix_cols(t)] = OWN[c, half, :]
        for d in [*hops, 0]:
            there = around(d)[0] * CORES
            dst = MIX.at[half, mix_cols(t)]
            if d:
                remote(OWN.at[c, half], dst, SX.at[2, d], RX.at[2, d], tp=there + c).start()
            remote(OWN.at[1 - c, half], dst, SD.at[2, d], RD.at[2, d], tp=there + 1 - c).start()

    blocks = [functools.partial(hidden_block, b) for b in range(nb)]
    next_tick()
    next_tick([nothing, state_before, blocks[0]])
    next_tick(blocks[1:])
    next_tick([pass_on, nothing])
    next_tick([nothing, project_ready])

    SSQ[...] = jnp.zeros_like(SSQ)

    def project(n):
        at = slice(n * 256, (n + 1) * 256)
        branch = jnp.dot(MIX[...], WO[:, at], preferred_element_type=F32)
        mid = (RES[:, at].astype(F32) + branch).astype(BF16)
        MID[:, at] = mid
        wide = mid.astype(F32)
        SSQ[...] += wide[:, :128] * wide[:, :128] + wide[:, 128:] * wide[:, 128:]

    def normalize(n):
        at = slice(n * own_rows, (n + 1) * own_rows)
        rows = pl.ds(pl.multiple_of((n * CORES + c) * own_rows, own_rows), own_rows)
        mean_sq = jnp.sum(SSQ[at, :], axis=1, keepdims=True) / width
        NRM[rows, :] = (MID[at, :].astype(F32) * lax.rsqrt(mean_sq + NORM_EPS) * fng_ref[...]).astype(BF16)
        begin(NRM.at[rows, :], NRM.at[rows, :], SN.at[n], RN.at[n], tp=sib)

    def normed_ready():
        for n in range(nx):
            rows = pl.ds(pl.multiple_of((n * CORES + 1 - c) * own_rows, own_rows), own_rows)
            remote(NRM.at[rows, :], NRM.at[rows, :], SN.at[n], RN.at[n], tp=sib).wait_recv()

    n_cols = width // 256
    next_tick([functools.partial(project, n) for n in range(n_cols)])
    next_tick([functools.partial(normalize, n) for n in range(nx)])
    normed_ready()

    def group_of(k):
        return rem(gz + k, ng)

    turn = [0]
    for n in range(1, ng // 2):
        turn += [ng - n, n]
    turn += [ng // 2]

    def upward(ks, n, n_col, final):
        at = slice(n * n_col, (n + 1) * n_col)
        value = None
        for k in ks:
            rows = pl.ds(pl.multiple_of(group_of(k) * gcols, gcols), gcols)
            part = jnp.dot(NRM[:, rows], UP[rows, at], preferred_element_type=F32)
            value = part if value is None else value + part
        if final:
            value = jnp.maximum(value + UACC[:, at], 0.0)
            ACT[:, at] = (value * value).astype(BF16)
        else:
            UACC[:, at] = value

    near = 2 * ((n_right - SUB) // SUB) - 1
    if share:
        for k in turn[:near]:
            from_pair(0, k)
    next_tick([functools.partial(upward, turn[:near], n, 128, False) for n in range(hid // 128)])
    while at_tick < n_right:
        next_tick()
    if share:
        for k in turn[near:]:
            from_pair(0, k)
    for n in range(hid // 256):
        upward(turn[near:], n, 256, True)

    def down(k):
        if share:
            from_pair(1, k)
        rows = pl.ds(pl.multiple_of(group_of(k) * gcols, gcols), gcols)
        value = lax.dot_general(
            ACT[...], DN[rows, :], (((1,), (1,)), ((), ())), preferred_element_type=F32
        )
        PART[k] = value.astype(BF16).reshape(nx, CORES, own_rows, gcols)
        copy = remote(PART.at[k, :, 1 - c], SIB.at[k], SP.at[k], RP.at[k], tp=sib)
        copy.start()
        waits.append(copy)

    def add_up(k):
        remote(SIB.at[k], SIB.at[k], SP.at[k], RP.at[k], tp=sib).wait_recv()
        for i in range(nx):
            SUM[k, i] = (PART[k, i, c].astype(F32) + SIB[k, i].astype(F32)).astype(BF16)
        for d in [2, 1, 3, *range(4, nx)]:
            if d < nx:
                i = rem(x + d, nx)
                copy = remote(SUM.at[k, i], RSR.at[k, x], SQ.at[k, d], RQ.at[k, d], tp=i * CORES + c)
                copy.start()
                waits.append(copy)

    def finish(k):
        at = pl.ds(pl.multiple_of(group_of(k) * gcols, gcols), gcols)
        value = MID[pl.ds(pl.multiple_of(x * own_rows, own_rows), own_rows), at].astype(F32)
        value = value + SUM[k, x].astype(F32)
        for d in range(1, nx):
            slot = RSR.at[k, rem(x - d + nx, nx)]
            remote(slot, slot, SQ.at[k, d], RQ.at[k, d], tp=sib).wait_recv()
            value = value + RSR[k, rem(x - d + nx, nx)].astype(F32)
        out_ref[:, at] = value.astype(BF16)

    for n, k in enumerate(turn):
        down(k)
        if n > 1:
            add_up(turn[n - 2])
        if n > 4:
            finish(turn[n - 5])
    for k in turn[-2:]:
        add_up(k)
    for k in turn[ng - 5 :]:
        finish(k)

    for ph, i in order:
        n_col, shared = cuts[ph][i][2:]
        cols = pl.ds(0, n_col)
        drain(weights[ph].at[pl.ds(0, n_right * UNIT), cols], SR.at[ph, i])
        drain(weights[ph].at[pl.ds(0, n_left * UNIT), cols], SL.at[ph, i])
        if shared:
            drain(weights[ph].at[pl.ds(0, (nz - 1) * UNIT), cols], SY.at[ph, i])
    for copy in waits:
        copy.wait_send()
    for d in range(1, SUB):
        drain(CS.at[0], SC.at[d])
    for d in range(nx):
        if d:
            drain(OWN.at[0], SX.at[2, d])
        drain(OWN.at[0], SD.at[2, d])

    @pl.when(gz < ng - 1)
    def _():
        drain(BS, SB.at[0])


def shards(
    sizes,
    queries,
    memory_keys,
    memory_values,
    output_preactivation,
    input_preactivation,
    forget_preactivation,
    extra_forget_terms,
    head_norm_gain,
    output_projection_matrix,
    residual,
    feedforward_norm_gain,
    feedforward_up_matrix,
    feedforward_down_matrix,
):
    nz, nt, share = sizes
    nx, ng = nt // CORES, nz // SUB
    tok, dh = queries.shape
    own_rows, width = residual.shape
    wrows, hid = feedforward_up_matrix.shape
    n_right = nz // 2
    n_pieces = 3 if share else 4
    gcols = SUB * wrows
    msg = (dh // SUB + 8, dh)
    dma = pltpu.SemaphoreType.DMA
    vmem = pltpu.VMEM
    scratch = [
        vmem((nz * wrows, hid), BF16),
        vmem((nz * wrows, hid), BF16),
        vmem((nt * dh, width), BF16),
        vmem((nx * own_rows, width), BF16),
        vmem((CORES, nx * own_rows, dh), BF16),
        vmem((nx * own_rows, nt * dh), BF16),
        vmem((nx * own_rows, width), BF16),
        vmem((tok, width), BF16),
        vmem((nx * own_rows, 128), F32),
        vmem((tok, hid), F32),
        vmem((tok, hid), BF16),
        vmem((ng, nx, CORES, own_rows, gcols), BF16),
        vmem((ng, nx, own_rows, gcols), BF16),
        vmem((ng, nx, own_rows, gcols), BF16),
        vmem((ng, nx, own_rows, gcols), BF16),
        vmem((tok // BLOCK - 1, dh, dh), F32),
        vmem((24, BLOCK), F32),
        vmem((SUB, *msg), F32),
        vmem((SUB, *msg), F32),
        vmem(msg, F32),
        vmem(msg, F32),
        vmem(msg, F32),
        vmem((SUB, *msg), F32),
        vmem((SUB, *msg), F32),
        dma((2, n_pieces)),
        dma((2, n_pieces, n_right + 1)),
        dma((2, n_pieces)),
        dma((2, n_pieces, n_right + 1)),
        dma((2, n_pieces)),
        dma((2, n_pieces, ng)),
        dma((3, nx)),
        dma((3, nx)),
        dma((3, nx)),
        dma((3, nx)),
        dma((nx,)),
        dma((nx,)),
        dma((SUB,)),
        dma((SUB,)),
        dma((1,)),
        dma((1,)),
        dma((SUB,)),
        dma((SUB,)),
        dma((ng,)),
        dma((ng,)),
        dma((ng, nx)),
        dma((ng, nx)),
        pltpu.SemaphoreType.REGULAR,
    ]
    return pl.pallas_call(
        functools.partial(kernel, sizes),
        out_shape=jax.ShapeDtypeStruct((own_rows, width), BF16),
        in_specs=[pl.BlockSpec(memory_space=pltpu.VMEM)] * 13,
        out_specs=pl.BlockSpec(memory_space=pltpu.VMEM),
        scratch_shapes=scratch,
        compiler_params=pltpu.CompilerParams(
            collective_id=0, has_side_effects=True, vmem_limit_bytes=56 * 1024 * 1024
        ),
        name="layer",
    )(
        queries,
        memory_keys,
        memory_values,
        output_preactivation,
        input_preactivation,
        forget_preactivation,
        extra_forget_terms,
        head_norm_gain.reshape(1, -1),
        output_projection_matrix,
        residual,
        feedforward_norm_gain.reshape(1, -1),
        feedforward_up_matrix,
        feedforward_down_matrix.T,
    )


def solution(mesh):
    in_specs = (
        P(("grp", "sp"), "tp"),
        P(("grp", "sp"), "tp"),
        P(("grp", "sp"), "tp"),
        P(("grp", "sp"), "tp"),
        P("tp", ("grp", "sp")),
        P("tp", ("grp", "sp")),
        P("tp", ("grp", "sp")),
        P(),
        P("tp", None),
        P(("grp", "sp", "tp"), None),
        P(),
        P("sp", "tp"),
        P("tp", "sp"),
    )
    out_specs = P(("grp", "sp", "tp"), None)
    sizes = (mesh.shape["sp"], mesh.shape["tp"], mesh.shape["grp"] % 2 == 0)
    return jax.shard_map(
        functools.partial(shards, sizes), mesh=mesh, in_specs=in_specs, out_specs=out_specs, check_vma=False
    )
```
